32 devices in a mesh: grp: 2 (over y), ep: 4 (over z), tp: 4 (over x, core).
Axes of the slice: x: 2, y: 2, z: 4, core: 2. Of those that a mesh axis runs over, the one named last changes fastest.
Arguments:
- memory_query_rows: bfloat16 [1024, 1024], P(('grp', 'ep'), 'tp'), parts along dimension 0, may hold values from -6 to 6
- memory_key_rows: bfloat16 [1024, 1024], P(('grp', 'ep'), 'tp'), parts along dimension 0, may hold values from -6 to 6
- memory_value_rows: bfloat16 [1024, 1024], P(('grp', 'ep'), 'tp'), parts along dimension 0, may hold values from -6 to 6
- input_gate_log: float32 [8, 1024], P('tp', ('grp', 'ep')), parts along dimension 1, may hold values from -4 to 300
- forget_gate_logits: float32 [8, 1024], P('tp', ('grp', 'ep')), parts along dimension 1
- forget_log_extra: float32 [8, 1024], P('tp', ('grp', 'ep')), parts along dimension 1, may hold values from -1.5 to 0
- memory_output_weight: bfloat16 [1024, 2048], P(None, 'tp'), may hold values from -0.1875 to 0.1875
- second_batch_tokens: bfloat16 [4096, 2048], P(('grp', 'ep', 'tp')), parts along dimension 0, may hold values from -6 to 6
- expert_norm_gain: float32 [2048], replicated, may hold values from 0.1 to 1.9
- routing_expert_index: int32 [4096, 2], P(('grp', 'ep', 'tp')), parts along dimension 0, may hold values from 0 to 3, all different within a row; in each aligned block of 128 rows (0 to 127, 128 to 255, ...) at most 80 rows name the same one
- routing_expert_weight: float32 [4096, 2], P(('grp', 'ep', 'tp')), parts along dimension 0, may hold values from 0.2 to 1
- expert_gate_matrix: bfloat16 [4, 2048, 3584], P('ep', None, 'tp'), may hold values from -0.125 to 0.125
- expert_up_matrix: bfloat16 [4, 2048, 3584], P('ep', None, 'tp'), may hold values from -0.125 to 0.125
- expert_down_matrix: bfloat16 [4, 3584, 2048], P('ep', 'tp'), may hold values from -0.09375 to 0.09375
Outputs:
- mixed_out: bfloat16 [1024, 2048], P(('grp', 'ep'), 'tp'), parts along dimension 0
- expert_out: bfloat16 [4096, 2048], P(('grp', 'ep', 'tp')), parts along dimension 0
The draws below stay inside these ranges and needn't reach their ends.
There are 2 independent parts, one for each index of `grp`. The reference program is written for one: setup_inputs(seed, part) draws one part's arguments, and reference() takes and returns one part's arrays. A program takes and returns all parts, laid end to end along the dimension named above; an argument that names none is the same for every part. Nothing has to cross between parts.
Inputs may be any that keep to these rules, and one draw needn't show every extreme that they name: `routing_expert_index`: within the rows of one device no expert is named by more than 80 rows, a bound that some block reaches; the 2 experts of a row differ.
All inputs are finite; a program needn't handle non-finite values.
Results may differ from the reference program's by a relative error of at most 0.012.
The reference program's roundings to bfloat16 on the way count: a program that leaves them out, or rounds other values in their place, can miss the bound.
Values may be sent and summed in bfloat16 or wider, within the bound.
A program may use at most 128 MiB of HBM per device.

```python
import math
import jax
import jax.numpy as jnp
import numpy as np
from jax import lax

D = 2048
HM = 8
DH = 128
FFE = 3584
TOP = 2
BLOCK = 128
TOK_A_EP = 128
TOK_B_DEV = 128
SEQ_LEN = 512
TOKENS_B = 2048
EXPERTS = 4
CAP = 80
N_TP = 4


def draw_input_gate_log(key, part):
    keys = jax.random.split(key, 1)
    base = jax.random.truncated_normal(keys[0], -4.0, 4.0, (HM, SEQ_LEN), jnp.float32)
    return base.astype(jnp.float32)


def draw_forget_gate_logits(key, part):
    keys = jax.random.split(key, 4)
    threshold = 0.5
    fast = jax.random.uniform(keys[0], (HM,), jnp.float32) < threshold
    fast_rate = 1.0 / jax.random.uniform(keys[1], (HM,), jnp.float32, 30.0, 100.0)
    slow_rate = 0.3 / SEQ_LEN
    rate = jnp.where(fast, fast_rate, slow_rate)
    factor = jnp.exp(jax.random.uniform(keys[2], (HM, SEQ_LEN // TOK_A_EP), jnp.float32, -0.7, 0.7))
    factor = jnp.repeat(factor, TOK_A_EP, axis=1)
    noise = 0.5 * jax.random.truncated_normal(keys[3], -4.0, 4.0, (HM, SEQ_LEN), jnp.float32)
    return (-jnp.log(jnp.expm1(rate[:, None] * factor)) + noise).astype(jnp.float32)


def draw_forget_log_extra(key, part):
    keys = jax.random.split(key, 2)
    places = jax.random.randint(keys[0], (HM, 3), 0, SEQ_LEN)
    amounts = jnp.log(jax.random.uniform(keys[1], (HM, 3), jnp.float32, 0.5, 0.8))
    spots = jnp.arange(SEQ_LEN, dtype=jnp.int32)[None, :]
    result = jnp.zeros((HM, SEQ_LEN), jnp.float32)
    for column in range(3):
        result = result + jnp.where(spots == places[:, column:column + 1], amounts[:, column:column + 1], 0.0)
    return result.astype(jnp.float32)


def block_levels(own_key, shape, cuts, low, top_value):
    loudness, own = 1.0, jax.random.fold_in(own_key, 6)
    for axis_at, parts in cuts:
        draws = jnp.exp(jax.random.uniform(jax.random.fold_in(own, axis_at), (parts,), jnp.float32, low / len(cuts), top_value / len(cuts)))
        loudness = loudness * jnp.repeat(draws, shape[axis_at] // parts).reshape([-1 if axis == axis_at else 1 for axis in range(len(shape))])
    return loudness


def shared_out(own_key, own, number, rows, amount, top, reach, lean):
    sequence = jax.random.permutation(own_key, amount)
    packed, usual = load_shares(amount, rows * top, reach, lean, True), load_shares(amount, rows * top, reach, lean, False)
    places = jnp.arange(amount)

    def named(lengths, offset_by):
        used = int((lengths > 0).sum())
        fixed = max(1, used // 4)
        passed = fixed + (places - fixed + offset_by * (used - fixed)) % max(1, amount - fixed)
        return jnp.zeros((amount,), jnp.int32).at[sequence[jnp.where(places < fixed, places, passed)]].set(jnp.asarray(lengths, jnp.int32))

    lengths = jnp.where(number % 4 == 0, named(packed, number // 4), named(usual, number - number // 4 - 1))
    mixed = jax.random.permutation(jax.random.fold_in(own, 3), amount)
    giver, sink = mixed[0:amount // 2 * 2:2], mixed[1:amount // 2 * 2:2]
    margin = jnp.minimum(lengths[giver] - 1, reach - lengths[sink]) // 2
    margin = jnp.where((giver == sequence[0]) | (sink == sequence[0]) | (lengths[sink] == 0), 0, jnp.maximum(margin, 0))
    passed = jax.random.randint(jax.random.fold_in(own, 4), (amount // 2,), 0, 1 << 20) % (margin + 1)
    lengths = lengths.at[giver].add(-passed).at[sink].add(passed)
    items = jnp.searchsorted(jnp.cumsum(lengths), jnp.arange(rows * top), side="right").astype(jnp.int32)
    grid = items.reshape(top, rows).T
    grid = grid[jax.random.permutation(jax.random.fold_in(own, 1), rows)]
    offset_by = jax.random.randint(jax.random.fold_in(own, 2), (rows, 1), 0, top)
    return jnp.take_along_axis(grid, (jnp.arange(top)[None, :] + offset_by) % top, axis=1)


def load_shares(count, total, reach, lean, full):
    loads = [(1 << 20) // math.isqrt(rank ** lean) + 1 for rank in range(1, count + 1)]
    largest = reach if full else min(reach, max(-(-total // count), total * loads[0] // sum(loads)))
    least = 1 if total - largest >= count - 1 else 0
    given, spare = [largest] + [least] * (count - 1), total - largest - least * (count - 1)
    while spare > 0:
        free = [i for i in range(1, count) if given[i] < largest] or [i for i in range(1, count) if given[i] < reach]
        whole, left = sum([loads[i] for i in free]), spare
        for i in free:
            addition = min(reach - given[i], max(1, left * loads[i] // whole), spare)
            given[i] = given[i] + addition
            spare = spare - addition
    return np.array(given)


def bell_draw(key, dims, scale, bound, pieces=(), held_as=jnp.bfloat16):
    values = jax.random.normal(key, dims, jnp.float32) * scale
    if len(pieces) > 0:
        values = block_levels(key, dims, pieces, -0.22, 0.18) * values
    return jnp.clip(values, min=-bound, max=bound).astype(held_as)


def setup_inputs(seed: int = 0, part: int = 0) -> dict:
    seeds = jax.random.split(jax.random.key(seed), 15)
    part_splits = jax.random.split(jax.random.fold_in(seeds[14], part), 15)
    memory_query_rows = bell_draw(part_splits[0], (SEQ_LEN, HM * DH), 1.0, 6.0, ((0, 4), (1, 4)))
    memory_key_rows = bell_draw(part_splits[1], (SEQ_LEN, HM * DH), 1.0, 6.0, ((0, 4), (1, 4)))
    memory_value_rows = bell_draw(part_splits[2], (SEQ_LEN, HM * DH), 1.0, 6.0, ((0, 4), (1, 4)))
    input_gate_log = draw_input_gate_log(jax.random.fold_in(jax.random.fold_in(seeds[14], part), 71), part)
    forget_gate_logits = draw_forget_gate_logits(jax.random.fold_in(jax.random.fold_in(seeds[14], part), 71), part)
    forget_log_extra = draw_forget_log_extra(jax.random.fold_in(jax.random.fold_in(seeds[14], part), 71), part)
    memory_output_weight = bell_draw(seeds[6], (HM * DH, D), (HM * DH) ** -0.5, 0.1875, ((1, 4),))
    second_batch_tokens = bell_draw(part_splits[7], (TOKENS_B, D), 1.0, 6.0, ((0, 16),))
    expert_norm_gain = jnp.clip(1.0 + 0.18 * jax.random.normal(seeds[8], (D,), jnp.float32), 0.1, 1.9)
    routing_expert_index_keys = jax.random.split(jax.random.fold_in(part_splits[9], 1), TOKENS_B // TOK_B_DEV)
    routing_expert_index_turns = jax.random.permutation(jax.random.fold_in(part_splits[9], 3), TOKENS_B // TOK_B_DEV)
    routing_expert_index = jax.vmap(lambda own, number: shared_out(jax.random.fold_in(part_splits[9], 2), own, number, TOK_B_DEV, EXPERTS, TOP, CAP, 1))(routing_expert_index_keys, routing_expert_index_turns).reshape((TOKENS_B, TOP))
    routing_expert_weight = jnp.clip(0.2 + 0.8 * jax.random.uniform(part_splits[10], (TOKENS_B, TOP), jnp.float32) ** block_levels(part_splits[10], (TOKENS_B, TOP), ((0, 16),), -0.2, 0.2), 0.2, 1.0)
    expert_gate_matrix = bell_draw(seeds[11], (EXPERTS, D, FFE), D ** -0.5, 0.125, ((0, 4), (2, 4)))
    expert_up_matrix = bell_draw(seeds[12], (EXPERTS, D, FFE), D ** -0.5, 0.125, ((0, 4), (2, 4)))
    expert_down_matrix = bell_draw(seeds[13], (EXPERTS, FFE, D), FFE ** -0.5, 0.09375, ((0, 4), (1, 4)))
    return {"memory_query_rows": memory_query_rows, "memory_key_rows": memory_key_rows, "memory_value_rows": memory_value_rows, "input_gate_log": input_gate_log, "forget_gate_logits": forget_gate_logits, "forget_log_extra": forget_log_extra, "memory_output_weight": memory_output_weight, "second_batch_tokens": second_batch_tokens, "expert_norm_gain": expert_norm_gain, "routing_expert_index": routing_expert_index, "routing_expert_weight": routing_expert_weight, "expert_gate_matrix": expert_gate_matrix, "expert_up_matrix": expert_up_matrix, "expert_down_matrix": expert_down_matrix}


rms_eps = 1e-06
highest = lax.Precision.HIGHEST

def state_update(state_in, inputs, cumulative):
    memory, normer, stabilizer = state_in
    key_rows, values, in_gate, forget = inputs
    block_total = cumulative[:, -1]
    weights = block_total[:, None] - cumulative + in_gate
    new_stab = jnp.maximum(block_total + stabilizer, lax.optimization_barrier(jnp.max(weights, axis=-1)))
    scaled = jnp.exp(weights - new_stab[:, None])
    retained = jnp.exp(block_total + stabilizer - new_stab)
    weighted_keys = scaled[:, :, None] * key_rows
    memory = retained[:, None, None] * memory + jnp.einsum('hsd,hse->hde', weighted_keys, values, precision=highest)
    normer = retained[:, None] * normer + lax.optimization_barrier(jnp.sum(weighted_keys, axis=1))
    return (memory, normer, new_stab)

def block_step(state_in, inputs):
    memory, normer, stabilizer = state_in
    queries, key_rows, values, in_gate, forget = inputs
    length = queries.shape[1]
    causal = jnp.tril(jnp.ones((length, length), dtype=bool))
    cumulative = jnp.cumsum(forget, axis=-1)
    decays = jnp.where(causal, cumulative[:, :, None] - cumulative[:, None, :] + in_gate[:, None, :], -jnp.inf)
    carried_max = cumulative + stabilizer[:, None]
    row_max = jnp.maximum(lax.optimization_barrier(jnp.max(decays, axis=-1)), carried_max)
    scores = jnp.einsum('htd,hsd->hts', queries, key_rows, precision=highest) * jnp.exp(decays - row_max[:, :, None])
    carried = jnp.exp(carried_max - row_max)
    numerator = carried[:, :, None] * jnp.einsum('htd,hde->hte', queries, memory, precision=highest) + jnp.einsum('hts,hse->hte', scores, values, precision=highest)
    denominator = carried * jnp.einsum('htd,hd->ht', queries, normer, precision=highest) + lax.optimization_barrier(jnp.sum(scores, axis=-1))
    output = numerator / jnp.maximum(jnp.abs(denominator), jnp.exp(-row_max))[:, :, None]
    new_state = state_update(state_in, (key_rows, values, in_gate, forget), cumulative)
    return (new_state, output)

def split_blocks(row_block, heads):
    count = row_block.shape[0] // BLOCK
    return row_block.astype(jnp.float32).reshape(count, BLOCK, heads, -1).transpose(0, 2, 1, 3)

def gate_blocks(gate_rows):
    heads = gate_rows.shape[0]
    return gate_rows.reshape(heads, -1, BLOCK).transpose(1, 0, 2)

def expert_ffn(row_block, gate_weight, up_weight, down_weight):
    gate_act = jnp.dot(row_block, gate_weight, preferred_element_type=jnp.float32)
    up_act = jnp.dot(row_block, up_weight, preferred_element_type=jnp.float32)
    hidden = (jax.nn.silu(gate_act) * up_act).astype(jnp.bfloat16)
    group_width = FFE // N_TP
    running = jnp.zeros((row_block.shape[0], D), jnp.float32)
    for group in range(N_TP):
        part_rows = hidden[:, group * group_width:(group + 1) * group_width]
        part_down = down_weight[group * group_width:(group + 1) * group_width]
        partial_out = jnp.dot(part_rows, part_down, preferred_element_type=jnp.float32).astype(jnp.bfloat16)
        running = running + partial_out.astype(jnp.float32)
    return running.astype(jnp.bfloat16)

def reference(memory_query_rows, memory_key_rows, memory_value_rows, input_gate_log, forget_gate_logits, forget_log_extra, memory_output_weight, second_batch_tokens, expert_norm_gain, routing_expert_index, routing_expert_weight, expert_gate_matrix, expert_up_matrix, expert_down_matrix):
    queries = split_blocks(memory_query_rows, HM)
    key_rows = split_blocks(memory_key_rows, HM) * DH ** (-0.5)
    values = split_blocks(memory_value_rows, HM)
    forget_log_value = jax.nn.log_sigmoid(forget_gate_logits) + forget_log_extra
    start_state = (jnp.zeros((HM, DH, DH), jnp.float32), jnp.zeros((HM, DH), jnp.float32), jnp.zeros((HM,), jnp.float32))
    _, outputs = lax.scan(block_step, start_state, (queries, key_rows, values, gate_blocks(input_gate_log), gate_blocks(forget_log_value)))
    memory_rows = outputs.transpose(0, 2, 1, 3).reshape(SEQ_LEN, HM * DH).astype(jnp.bfloat16)
    mixed_out = jnp.dot(memory_rows, memory_output_weight, preferred_element_type=jnp.float32).astype(jnp.bfloat16)
    tokens_f = second_batch_tokens.astype(jnp.float32)
    normed = (tokens_f * lax.rsqrt(lax.optimization_barrier(jnp.mean(tokens_f * tokens_f, axis=1, keepdims=True)) + rms_eps) * expert_norm_gain).astype(jnp.bfloat16)
    devices = TOKENS_B // TOK_B_DEV
    flat_ids = routing_expert_index.reshape(devices, TOK_B_DEV * TOP)
    onehot = (flat_ids[:, :, None] == jnp.arange(EXPERTS, dtype=jnp.int32)[None, None, :]).astype(jnp.int32)
    route_ranks = lax.optimization_barrier(jnp.sum((jnp.cumsum(onehot, axis=1) - 1) * onehot, axis=2))
    owner = jnp.arange(devices, dtype=jnp.int32)[:, None]
    slot_ids = (flat_ids * (devices * CAP) + owner * CAP + route_ranks).reshape(-1).astype(jnp.int32)
    token_ids = jnp.repeat(jnp.arange(TOKENS_B, dtype=jnp.int32), TOP)
    slot_table = jnp.full((EXPERTS * devices * CAP,), TOKENS_B, jnp.int32).at[slot_ids].set(token_ids)
    padded = jnp.concatenate([normed, jnp.zeros((1, D), jnp.bfloat16)], axis=0)

    def one_expert(inputs):
        index_rows, gate_weight, up_weight, down_weight = inputs
        return expert_ffn(padded[index_rows], gate_weight, up_weight, down_weight)
    results = lax.map(one_expert, (slot_table.reshape(EXPERTS, devices * CAP), expert_gate_matrix, expert_up_matrix, expert_down_matrix))
    picked = results.reshape(-1, D)[slot_ids].astype(jnp.float32).reshape(TOKENS_B, TOP, D)
    expert_out = lax.optimization_barrier(jnp.sum(picked * routing_expert_weight[:, :, None], axis=1)).astype(jnp.bfloat16)
    return (mixed_out, expert_out)
```

```python
import functools

import jax
import jax.numpy as jnp
from jax import lax
from jax.experimental import pallas as pl
from jax.experimental.pallas import tpu as pltpu
from jax.sharding import PartitionSpec as P

DH = 128
TOP = 2

rms_eps = 1e-06
highest = lax.Precision.HIGHEST


MESH = pl.DeviceIdType.MESH
LANES = 128
GROUP = 16


def pieces(cap):
    half = -(-cap // 32) * 16
    return [(0, half), (half, cap - half)] if cap > half else [(0, cap)]


def fused_kernel(
    ep,
    tp,
    cap,
    query_hbm,
    key_hbm,
    value_hbm,
    in_gate_ref,
    logit_ref,
    extra_ref,
    mix_hbm,
    token_hbm,
    gain_ref,
    index_ref,
    weight_ref,
    gate_hbm,
    up_hbm,
    down_hbm,
    mixed_ref,
    out_ref,
    query_ref,
    key_ref,
    value_ref,
    tokens,
    normed,
    send,
    slot_row,
    slot_col,
    weight_col,
    gate_up,
    down,
    rows,
    hidden,
    part,
    near_part,
    pair_sum,
    far_part,
    result,
    returned,
    total_out,
    local_state,
    state_in,
    state_out,
    memory,
    mix,
    w_sem,
    own_sem,
    st_sem,
    z_sem,
    far_sem,
    near_sem,
    relay_sem,
    no_sem,
    nf_sem,
    fp_sem,
    r_sem,
    m_sem,
    go_sem,
):
    e = lax.axis_index("ep")
    t = lax.axis_index("tp")
    side, core = t // 2, t % 2
    near = side * 2 + (1 - core)
    far = (1 - side) * 2 + core
    across = (1 - side) * 2 + (1 - core)
    heads = in_gate_ref.shape[0]
    length = in_gate_ref.shape[1]
    tiles = gate_up.shape[0]
    width = rows.shape[2]
    tok_rows = tokens.shape[0]
    cuts = pieces(cap)
    count = range(len(cuts))
    line = ep == 4

    if line:
        left = 1 - e // 2
        inner = e * left + (3 - e) * (1 - left)

        def seat(v):
            return v * left + (3 - v) * (1 - left)

        targets = [e, seat(1 + 2 * inner), seat(3 - inner), seat(2 - 2 * inner)]
        sources = [e, targets[3], targets[2], targets[1]]
        gathers = [e, seat(3), seat(2), seat(1 - inner)]
    else:
        targets = [lax.rem(e + k, ep) for k in range(ep)]
        sources = [lax.rem(e + ep - k, ep) for k in range(ep)]
        gathers = targets

    def block(side_at, core_at, p=None):
        off, size = (0, cap) if p is None else cuts[p]
        return pl.ds(pl.multiple_of((side_at * 2 + core_at) * cap + off, GROUP), size)

    def cut(p):
        return pl.ds(cuts[p][0], cuts[p][1])

    def remote(src, dst, sent, received, target):
        return pltpu.make_async_remote_copy(
            src_ref=src,
            dst_ref=dst,
            send_sem=sent,
            recv_sem=received,
            device_id=target,
            device_id_type=MESH,
        )

    def weight_copies(i):
        cols = pl.ds(pl.multiple_of(i * LANES, LANES), LANES)
        return (
            pltpu.make_async_copy(
                gate_hbm.at[0, :, cols], gate_up.at[i, :, pl.ds(0, LANES)], w_sem.at[0, i]
            ),
            pltpu.make_async_copy(
                up_hbm.at[0, :, cols], gate_up.at[i, :, pl.ds(LANES, LANES)], w_sem.at[1, i]
            ),
        )

    token_copy = pltpu.make_async_copy(token_hbm, tokens, own_sem.at[0])
    down_copy = pltpu.make_async_copy(down_hbm.at[0], down, own_sem.at[1])
    mix_copy = pltpu.make_async_copy(mix_hbm, mix, own_sem.at[2])
    head_copies = [
        pltpu.make_async_copy(query_hbm, query_ref, own_sem.at[3]),
        pltpu.make_async_copy(key_hbm, key_ref, own_sem.at[4]),
        pltpu.make_async_copy(value_hbm, value_ref, own_sem.at[5]),
    ]

    def z_send(s, p):
        return remote(
            send.at[s, cut(p)], rows.at[e, block(side, core, p)],
            z_sem.at[0, s, p], z_sem.at[1, e, p], {"ep": s},
        )

    def z_recv(s, p):
        return remote(
            send.at[s, cut(p)], rows.at[s, block(side, core, p)],
            z_sem.at[0, s, p], z_sem.at[1, s, p], {"ep": s},
        )

    def mine_copy(s, p, sems, target):
        span = rows.at[s, block(side, core, p)]
        return remote(span, span, sems.at[0, s, p], sems.at[1, s, p], {"tp": target})

    def far_copy(s, p):
        return mine_copy(s, p, far_sem, far)

    def near_copy(s, p):
        return mine_copy(s, p, near_sem, near)

    def relay_copy(s, p):
        span = rows.at[s, block(1 - side, core, p)]
        return remote(span, span, relay_sem.at[0, s, p], relay_sem.at[1, s, p], {"tp": near})

    def near_own_copy(s):
        return remote(
            part.at[s, block(side, 1 - core)], near_part.at[s, 0],
            no_sem.at[0, s], no_sem.at[1, s], {"tp": near},
        )

    def near_far_copy(s):
        return remote(
            part.at[s, block(1 - side, 1 - core)], near_part.at[s, 1],
            nf_sem.at[0, s], nf_sem.at[1, s], {"tp": near},
        )

    def far_part_copy(s, p):
        return remote(
            pair_sum.at[s, cut(p)], far_part.at[s, cut(p)],
            fp_sem.at[0, s, p], fp_sem.at[1, s, p], {"tp": far},
        )

    def return_send(s, p):
        return remote(
            result.at[s, cut(p)], returned.at[e, cut(p)],
            r_sem.at[0, s, p], r_sem.at[1, e, p], {"ep": s},
        )

    def return_recv(s, p):
        return remote(
            result.at[s, cut(p)], returned.at[s, cut(p)],
            r_sem.at[0, s, p], r_sem.at[1, s, p], {"ep": s},
        )

    state_copy = remote(
        state_out, state_in, st_sem.at[0, 0], st_sem.at[1, 0], {"ep": lax.rem(e + 1, ep)}
    )

    def memory_copy(i):
        span = memory.at[far if i == 2 else t]
        return remote(
            span, span, m_sem.at[0, i], m_sem.at[1, i], {"tp": far if i == 1 else near}
        )

    def gates(h):
        logits = logit_ref[h : h + 1, :]
        forget = (
            jnp.minimum(logits, 0.0) - jnp.log1p(jnp.exp(-jnp.abs(logits)))
        ) + extra_ref[h : h + 1, :]
        at_row = lax.broadcasted_iota(jnp.int32, (length, length), 0)
        at_col = lax.broadcasted_iota(jnp.int32, (length, length), 1)
        diagonal = at_row == at_col
        in_row = in_gate_ref[h : h + 1, :]
        in_col = jnp.sum(jnp.where(diagonal, in_row, 0.0), axis=1, keepdims=True)
        sum_col = jnp.sum(jnp.where(at_col <= at_row, forget, 0.0), axis=1, keepdims=True)
        sum_row = jnp.sum(jnp.where(diagonal, sum_col, 0.0), axis=0, keepdims=True)
        total = jnp.sum(forget, axis=1, keepdims=True)
        return in_row, in_col, sum_row, sum_col, total, at_col <= at_row

    def head(ref, h):
        return ref[:, h * DH : (h + 1) * DH].astype(jnp.float32)

    def local_part():
        for h in range(heads):
            _, in_col, _, sum_col, total, _ = gates(h)
            weights = total - sum_col + in_col
            stab = jnp.max(weights, axis=0, keepdims=True)
            weighted = jnp.exp(weights - stab) * (head(key_ref, h) * DH ** (-0.5))
            local_state[h, 0:DH, :] = jnp.dot(
                weighted.T, head(value_ref, h), precision=highest,
                preferred_element_type=jnp.float32,
            )
            local_state[h, DH : DH + 1, :] = jnp.sum(weighted, axis=0, keepdims=True)
            local_state[h, DH + 1 : DH + 2, :] = jnp.broadcast_to(stab, (1, DH))
            local_state[h, DH + 2 : DH + 3, :] = jnp.broadcast_to(total, (1, DH))

    def pass_state():
        for h in range(heads):
            total = local_state[h, DH + 2 : DH + 3, :]
            stab_own = local_state[h, DH + 1 : DH + 2, :]
            carried = total + state_in[h, DH + 1 : DH + 2, :]
            stab = jnp.maximum(carried, stab_own)
            old, new = jnp.exp(carried - stab), jnp.exp(stab_own - stab)
            state_out[h, 0 : DH + 1, :] = (
                old * state_in[h, 0 : DH + 1, :] + new * local_state[h, 0 : DH + 1, :]
            )
            state_out[h, DH + 1 : DH + 2, :] = stab
        state_copy.start()

    def memory_part():
        for h in range(heads):
            in_row, _, sum_row, sum_col, _, causal = gates(h)
            decays = jnp.where(causal, sum_col - sum_row + in_row, -jnp.inf)
            carried_max = sum_col + state_in[h, DH + 1 : DH + 2, 0:1]
            row_max = jnp.maximum(jnp.max(decays, axis=1, keepdims=True), carried_max)
            queries = head(query_ref, h)
            keys = head(key_ref, h) * DH ** (-0.5)
            scores = jnp.dot(
                queries, keys.T, precision=highest, preferred_element_type=jnp.float32
            ) * jnp.exp(decays - row_max)
            carried = jnp.exp(carried_max - row_max)
            numerator = carried * jnp.dot(
                queries, state_in[h, 0:DH, :], precision=highest,
                preferred_element_type=jnp.float32,
            ) + jnp.dot(
                scores, head(value_ref, h), precision=highest,
                preferred_element_type=jnp.float32,
            )
            denominator = carried * jnp.sum(
                queries * state_in[h, DH : DH + 1, :], axis=1, keepdims=True
            ) + jnp.sum(scores, axis=1, keepdims=True)
            memory[t, :, h * DH : (h + 1) * DH] = (
                numerator / jnp.maximum(jnp.abs(denominator), jnp.exp(-row_max))
            ).astype(jnp.bfloat16)
        memory_copy(0).start()
        memory_copy(1).start()

    def mix_part():
        memory_copy(1).wait_recv()
        memory_copy(2).start()
        mix_copy.wait()
        memory_copy(0).wait_recv()
        memory_copy(2).wait_recv()
        total = jnp.zeros(mixed_ref.shape, jnp.float32)
        for i in range(tp):
            total = total + jnp.dot(
                memory[i], mix[i * heads * DH : (i + 1) * heads * DH, :],
                preferred_element_type=jnp.float32,
            )
        mixed_ref[...] = total.astype(jnp.bfloat16)

    def slots():
        at_row = lax.broadcasted_iota(jnp.int32, (tok_rows, tok_rows), 0)
        at_col = lax.broadcasted_iota(jnp.int32, (tok_rows, tok_rows), 1)
        chosen = [index_ref[c : c + 1, :] == at_row for c in range(TOP)]
        member = jnp.zeros((tok_rows, tok_rows), jnp.float32)
        weights = jnp.zeros((tok_rows, tok_rows), jnp.float32)
        for c in range(TOP):
            member = member + jnp.where(chosen[c], 1.0, 0.0)
            weights = weights + jnp.where(chosen[c], weight_ref[c : c + 1, :], 0.0)
        earlier = jnp.where(at_row < at_col, 1.0, 0.0).astype(jnp.bfloat16)
        ranks = jnp.dot(member.astype(jnp.bfloat16), earlier, preferred_element_type=jnp.float32)
        slot = jnp.where(member > 0.0, ranks, -1.0)
        slot_row[...] = slot
        slot_col[...] = slot.T
        weight_col[...] = weights.T

    def norm():
        @pl.loop(0, tok_rows // GROUP)
        def _(i):
            span = pl.ds(pl.multiple_of(i * GROUP, GROUP), GROUP)
            values = tokens[span].astype(jnp.float32)
            scale = lax.rsqrt(jnp.mean(values * values, axis=1, keepdims=True) + rms_eps)
            normed[span] = (values * scale * gain_ref[...]).astype(jnp.bfloat16)

    def dispatch(x, place):
        at_slot = lax.broadcasted_iota(jnp.int32, (cap, tok_rows), 0).astype(jnp.float32)
        taken = jnp.where(at_slot == slot_row[pl.ds(x, 1), :], 1.0, 0.0).astype(jnp.bfloat16)

        @pl.loop(0, width // 512)
        def _(i):
            cols = pl.ds(pl.multiple_of(i * 512, 512), 512)
            place[:, cols] = jnp.dot(
                taken, normed[:, cols], preferred_element_type=jnp.float32
            ).astype(jnp.bfloat16)

    def combine(x, first, last):
        lane = lax.broadcasted_iota(jnp.int32, (tok_rows, tok_rows), 1)
        slot = jnp.sum(jnp.where(lane == x, slot_col[...], 0.0), axis=1, keepdims=True)
        weight = jnp.sum(jnp.where(lane == x, weight_col[...], 0.0), axis=1, keepdims=True)
        at_slot = lax.broadcasted_iota(jnp.int32, (tok_rows, cap), 1).astype(jnp.float32)
        taken = jnp.where(at_slot == slot, 1.0, 0.0).astype(jnp.bfloat16)

        @pl.loop(0, width // 512)
        def _(i):
            cols = pl.ds(pl.multiple_of(i * 512, 512), 512)
            total = weight * jnp.dot(
                taken, returned[x, :, cols], preferred_element_type=jnp.float32
            )
            if not first:
                total = total + total_out[:, cols]
            if last:
                out_ref[:, cols] = total.astype(jnp.bfloat16)
            else:
                total_out[:, cols] = total

    def feed_forward(s, group, first=False):
        span = pl.ds(pl.multiple_of(group * 2 * cap, 2 * cap), 2 * cap)

        @pl.loop(0, tiles)
        def _(i):
            if first:
                for copy in weight_copies(i):
                    copy.wait()
            both = jnp.dot(rows[s, span], gate_up[i], preferred_element_type=jnp.float32)
            act, up_act = both[:, :LANES], both[:, LANES:]
            hidden[:, pl.ds(pl.multiple_of(i * LANES, LANES), LANES)] = (
                jax.nn.silu(act) * up_act
            ).astype(jnp.bfloat16)

        if first:
            down_copy.wait()

        @pl.loop(0, width // 256)
        def _(i):
            cols = pl.ds(pl.multiple_of(i * 256, 256), 256)
            part[s, span, cols] = jnp.dot(
                hidden[...], down[:, cols], preferred_element_type=jnp.float32
            ).astype(jnp.bfloat16)

    def gather_start(s, p):
        far_copy(s, p).start()
        near_copy(s, p).start()

    def arrive(j, which=None):
        for p in count if which is None else which:
            z_recv(sources[j], p).wait_recv()
            gather_start(sources[j], p)

    def own_group(j):
        s = sources[j]
        for p in count:
            near_copy(s, p).wait_recv()
        feed_forward(s, side, first=j == 0)
        near_own_copy(s).start()

    def relay(j):
        s = sources[j]
        for p in count:
            far_copy(s, p).wait_recv()
            relay_copy(s, p).start()

    def far_group(j):
        s = sources[j]
        for p in count:
            relay_copy(s, p).wait_recv()
        feed_forward(s, 1 - side)
        near_far_copy(s).start()

    def pair(j):
        s = sources[j]
        near_far_copy(s).wait_recv()
        base = (1 - side) * 2 * cap + core * cap
        for p in count:
            off, size = cuts[p]

            @pl.loop(0, size // GROUP)
            def _(i):
                at = pl.multiple_of(off + i * GROUP, GROUP)
                pair_sum[s, pl.ds(at, GROUP)] = (
                    part[s, pl.ds(pl.multiple_of(base + at, GROUP), GROUP)].astype(jnp.float32)
                    + near_part[s, 1, pl.ds(at, GROUP)].astype(jnp.float32)
                ).astype(jnp.bfloat16)

            far_part_copy(s, p).start()

    def finish(j, which=None):
        s = sources[j]
        base = side * 2 * cap + core * cap
        for p in count if which is None else which:
            if p == 0:
                near_own_copy(s).wait_recv()
            far_part_copy(s, p).wait_recv()
            off, size = cuts[p]

            @pl.loop(0, size // GROUP)
            def _(i):
                at = pl.multiple_of(off + i * GROUP, GROUP)
                total = (
                    part[s, pl.ds(pl.multiple_of(base + at, GROUP), GROUP)].astype(jnp.float32)
                    + near_part[s, 0, pl.ds(at, GROUP)].astype(jnp.float32)
                    + far_part[s, pl.ds(at, GROUP)].astype(jnp.float32)
                ).astype(jnp.bfloat16)
                if j == 0:
                    returned[s, pl.ds(at, GROUP)] = total
                else:
                    result[s, pl.ds(at, GROUP)] = total

            if j > 0:
                return_send(s, p).start()

    def gather_back(k):
        x = gathers[k]
        if k > 0:
            for p in count:
                return_recv(x, p).wait_recv()
        combine(x, k == 0, k == ep - 1)

    def start_send(k):
        for p in count:
            z_send(targets[k], p).start()

    def state_step():
        state_copy.wait_recv()

        @pl.when(e + 1 < ep)
        def _():
            pass_state()

    token_copy.start()
    for copy in head_copies:
        copy.start()

    @pl.loop(0, tiles)
    def _(i):
        for copy in weight_copies(i):
            copy.start()

    down_copy.start()
    mix_copy.start()
    barrier = pltpu.get_barrier_semaphore()

    @pl.loop(1, ep)
    def _(k):
        pl.semaphore_signal(
            barrier, inc=1, device_id={"ep": lax.rem(e + k, ep)}, device_id_type=MESH
        )

    for target in (near, far, across):
        pl.semaphore_signal(barrier, inc=1, device_id={"tp": target}, device_id_type=MESH)
    slots()
    token_copy.wait()
    norm()
    dispatch(e, rows.at[e, block(side, core)])
    pl.semaphore_wait(barrier, ep + 2)
    for p in count:
        gather_start(e, p)
    for k in range(1, ep):
        dispatch(targets[k], send.at[targets[k]])
        if k == 1 or not line:
            start_send(k)
        elif k == 2:
            pl.when(inner == 0)(functools.partial(start_send, 2))
    for copy in head_copies:
        copy.wait()
    local_part()

    @pl.when(e == 0)
    def _():
        state_in[...] = jnp.zeros_like(state_in)
        if ep > 1:
            pass_state()

    own_group(0)
    if line:
        arrive(1)
        relay(0)
        far_group(0)
        own_group(1)

        @pl.when(inner == 0)
        def _():
            arrive(2, count[:1])
            pl.semaphore_signal(
                go_sem, inc=1, device_id={"ep": lax.rem(e + 2, ep)}, device_id_type=MESH
            )
            arrive(2, count[1:])
            start_send(3)

        @pl.when(inner == 1)
        def _():
            pair(0)
            pl.semaphore_wait(go_sem, 1)
            start_send(2)
            start_send(3)

        relay(1)
        far_group(1)

        @pl.when(inner == 1)
        def _():
            arrive(2)
            pl.when(e == 1)(state_step)

        own_group(2)

        @pl.when(inner == 0)
        def _():
            pair(1)
            relay(2)

        @pl.when(inner == 1)
        def _():
            arrive(3, count[:1])
            relay(2)
            arrive(3, count[1:])

        far_group(2)

        @pl.when(inner == 0)
        def _():
            finish(1, count[:1])
            pair(2)
            arrive(3)
            finish(1, count[1:])

        own_group(3)

        @pl.when(inner == 0)
        def _():
            finish(2)
            pair(0)
            pl.when(e == ep - 1)(state_step)
            relay(3)

        @pl.when(inner == 1)
        def _():
            pair(2)
            finish(0)
            pl.when(e == 2)(state_step)
            relay(3)

        far_group(3)

        @pl.when(inner == 0)
        def _():
            pair(3)

        @pl.when(inner == 1)
        def _():
            finish(2, count[:1])
            pair(3)
            pair(1)
            finish(2, count[1:])

        memory_part()

        @pl.when(inner == 0)
        def _():
            finish(0)
            finish(3)

        @pl.when(inner == 1)
        def _():
            finish(3)
            finish(1)

        gather_back(0)
        gather_back(1)
        mix_part()
        gather_back(2)
        gather_back(3)
    else:
        for j in range(ep):
            if j + 1 < ep:
                arrive(j + 1)
            if j > 0:
                own_group(j)
            relay(j)
            far_group(j)
            if j > 0:
                pl.when(e == j)(state_step)
            pair(j)
            if j > 0:
                finish(j - 1)
        finish(ep - 1)
        memory_part()
        mix_part()
        for k in range(ep):
            gather_back(k)

    for i in range(3):
        memory_copy(i).wait_send()

    @pl.when(e + 1 < ep)
    def _():
        state_copy.wait_send()

    @pl.loop(0, ep)
    def _(s):
        near_own_copy(s).wait_send()
        near_far_copy(s).wait_send()
        for p in count:
            far_copy(s, p).wait_send()
            near_copy(s, p).wait_send()
            relay_copy(s, p).wait_send()
            far_part_copy(s, p).wait_send()

    @pl.loop(1, ep)
    def _(k):
        s = lax.rem(e + k, ep)
        for p in count:
            z_send(s, p).wait_send()
            return_send(s, p).wait_send()


def on_device(
    memory_query_rows,
    memory_key_rows,
    memory_value_rows,
    input_gate_log,
    forget_gate_logits,
    forget_log_extra,
    memory_output_weight,
    second_batch_tokens,
    expert_norm_gain,
    routing_expert_index,
    routing_expert_weight,
    expert_gate_matrix,
    expert_up_matrix,
    expert_down_matrix,
):
    ep, tp = lax.axis_size("ep"), lax.axis_size("tp")
    tok_rows, width = second_batch_tokens.shape
    capacity = max(2, 5 * tok_rows * TOP // (4 * ep))
    cap = -(-capacity // GROUP) * GROUP
    part_hidden = expert_gate_matrix.shape[2]
    tiles = part_hidden // LANES
    positions = memory_query_rows.shape[0]
    heads = input_gate_log.shape[0]
    bf16 = jnp.bfloat16
    vmem = pl.BlockSpec(memory_space=pltpu.VMEM)
    hbm = pl.BlockSpec(memory_space=pl.ANY)
    whole = pltpu.SemaphoreType.DMA((2, ep))
    split = pltpu.SemaphoreType.DMA((2, ep, len(pieces(cap))))
    state = pltpu.VMEM((heads, DH + 8, DH), jnp.float32)
    square = pltpu.VMEM((tok_rows, tok_rows), jnp.float32)
    slotted = pltpu.VMEM((ep, cap, width), bf16)
    head_rows = pltpu.VMEM(memory_query_rows.shape, bf16)
    token_rows = pltpu.VMEM((tok_rows, width), bf16)
    return pl.pallas_call(
        functools.partial(fused_kernel, ep, tp, cap),
        out_shape=(
            jax.ShapeDtypeStruct((positions, memory_output_weight.shape[1]), bf16),
            jax.ShapeDtypeStruct((tok_rows, width), bf16),
        ),
        in_specs=[hbm] * 3 + [vmem] * 3 + [hbm] * 2 + [vmem] * 3 + [hbm] * 3,
        out_specs=(vmem, vmem),
        scratch_shapes=[
            head_rows,
            head_rows,
            head_rows,
            token_rows,
            token_rows,
            slotted,
            square,
            square,
            square,
            pltpu.VMEM((tiles, width, 2 * LANES), bf16),
            pltpu.VMEM((part_hidden, width), bf16),
            pltpu.VMEM((ep, tp * cap, width), bf16),
            pltpu.VMEM((2 * cap, part_hidden), bf16),
            pltpu.VMEM((ep, tp * cap, width), bf16),
            pltpu.VMEM((ep, 2, cap, width), bf16),
            slotted,
            slotted,
            slotted,
            slotted,
            pltpu.VMEM((tok_rows, width), jnp.float32),
            state,
            state,
            state,
            pltpu.VMEM((tp, positions, heads * DH), bf16),
            pltpu.VMEM(memory_output_weight.shape, bf16),
            pltpu.SemaphoreType.DMA((2, tiles)),
            pltpu.SemaphoreType.DMA((6,)),
            pltpu.SemaphoreType.DMA((2, 1)),
            split,
            split,
            split,
            split,
            whole,
            whole,
            split,
            split,
            pltpu.SemaphoreType.DMA((2, 3)),
            pltpu.SemaphoreType.REGULAR,
        ],
        compiler_params=pltpu.CompilerParams(
            collective_id=0, has_side_effects=True, vmem_limit_bytes=66000000
        ),
        cost_estimate=pl.CostEstimate(
            flops=6 * ep * tp * cap * width * part_hidden,
            bytes_accessed=6 * width * part_hidden,
            transcendentals=ep * tp * cap * part_hidden,
        ),
    )(
        memory_query_rows,
        memory_key_rows,
        memory_value_rows,
        input_gate_log,
        forget_gate_logits,
        forget_log_extra,
        memory_output_weight,
        second_batch_tokens,
        expert_norm_gain.reshape(1, -1),
        routing_expert_index.T,
        routing_expert_weight.T,
        expert_gate_matrix,
        expert_up_matrix,
        expert_down_matrix,
    )


def solution(mesh):
    placed = (
        P(("grp", "ep"), "tp"),
        P(("grp", "ep"), "tp"),
        P(("grp", "ep"), "tp"),
        P("tp", ("grp", "ep")),
        P("tp", ("grp", "ep")),
        P("tp", ("grp", "ep")),
        P(None, "tp"),
        P(("grp", "ep", "tp"), None),
        P(),
        P(("grp", "ep", "tp"), None),
        P(("grp", "ep", "tp"), None),
        P("ep", None, "tp"),
        P("ep", None, "tp"),
        P("ep", "tp", None),
    )
    return jax.shard_map(
        on_device,
        mesh=mesh,
        in_specs=placed,
        out_specs=(P(("grp", "ep"), "tp"), P(("grp", "ep", "tp"), None)),
        check_vma=False,
    )
```

```python
import functools

import jax
import jax.numpy as jnp
from jax import lax
from jax.experimental import pallas as pl
from jax.experimental.pallas import tpu as pltpu
from jax.sharding import PartitionSpec as P

DH = 128
TOP = 2

rms_eps = 1e-06
highest = lax.Precision.HIGHEST


MESH = pl.DeviceIdType.MESH
LANES = 128
GROUP = 16


def pieces(cap):
    first = cap // 32 * 16
    return [(0, first), (first, cap - first)] if first else [(0, cap)]


def fused_kernel(
    ep,
    tp,
    cap,
    query_hbm,
    key_hbm,
    value_hbm,
    in_gate_ref,
    logit_ref,
    extra_ref,
    mix_hbm,
    token_hbm,
    gain_ref,
    index_ref,
    weight_ref,
    gate_hbm,
    up_hbm,
    down_hbm,
    mixed_ref,
    out_ref,
    query_ref,
    key_ref,
    value_ref,
    tokens,
    normed,
    send,
    slot_row,
    slot_col,
    weight_col,
    gate_up,
    down,
    rows,
    hidden,
    part,
    near_part,
    pair_sum,
    far_part,
    result,
    returned,
    total_out,
    local_state,
    state_in,
    state_out,
    memory,
    mix,
    w_sem,
    own_sem,
    st_sem,
    z_sem,
    far_sem,
    near_sem,
    relay_sem,
    no_sem,
    nf_sem,
    fp_sem,
    r_sem,
    m_sem,
    go_sem,
):
    e = lax.axis_index("ep")
    t = lax.axis_index("tp")
    side, core = t // 2, t % 2
    near = side * 2 + (1 - core)
    far = (1 - side) * 2 + core
    across = (1 - side) * 2 + (1 - core)
    heads = in_gate_ref.shape[0]
    length = in_gate_ref.shape[1]
    tiles = gate_up.shape[1] // (2 * LANES)
    width = rows.shape[2]
    part_hidden = down.shape[0]
    tok_rows = tokens.shape[0]
    cuts = pieces(cap)
    count = range(len(cuts))
    head, tail = count[:1], count[1:]
    line = ep == 4

    if line:
        left = 1 - e // 2
        inner = e * left + (3 - e) * (1 - left)

        def seat(v):
            return v * left + (3 - v) * (1 - left)

        targets = [e, seat(1 + 2 * inner), seat(3 - inner), seat(2 - 2 * inner)]
        sources = [e, targets[3], targets[2], targets[1]]

        def source(j):
            return sources[j]

        gathers = [e, seat(3), seat(2), seat(1 - inner)]
    else:
        targets = [lax.rem(e + k, ep) for k in range(ep)]
        gathers = targets

        def source(j):
            return lax.rem(e + ep - j, ep)

    def block(side_at, core_at, p=None):
        off, size = (0, cap) if p is None else cuts[p]
        return pl.ds(pl.multiple_of((side_at * 2 + core_at) * cap + off, GROUP), size)

    def cut(p):
        return pl.ds(cuts[p][0], cuts[p][1])

    def remote(src, dst, sent, received, target):
        return pltpu.make_async_remote_copy(
            src_ref=src,
            dst_ref=dst,
            send_sem=sent,
            recv_sem=received,
            device_id=target,
            device_id_type=MESH,
        )

    def pair_cols(i, which):
        return pl.ds(pl.multiple_of((2 * i + which) * LANES, LANES), LANES)

    def weight_copies(i):
        cols = pl.ds(pl.multiple_of(i * LANES, LANES), LANES)
        return (
            pltpu.make_async_copy(
                gate_hbm.at[0, :, cols], gate_up.at[:, pair_cols(i, 0)], w_sem.at[0, i]
            ),
            pltpu.make_async_copy(
                up_hbm.at[0, :, cols], gate_up.at[:, pair_cols(i, 1)], w_sem.at[1, i]
            ),
        )

    token_copy = pltpu.make_async_copy(token_hbm, tokens, own_sem.at[0])
    down_copy = pltpu.make_async_copy(down_hbm.at[0], down, own_sem.at[1])
    mix_copy = pltpu.make_async_copy(mix_hbm, mix, own_sem.at[2])
    head_copies = [
        pltpu.make_async_copy(query_hbm, query_ref, own_sem.at[3]),
        pltpu.make_async_copy(key_hbm, key_ref, own_sem.at[4]),
        pltpu.make_async_copy(value_hbm, value_ref, own_sem.at[5]),
    ]

    def z_send(s, p):
        return remote(
            send.at[s, cut(p)], rows.at[e, block(side, core, p)],
            z_sem.at[0, s, p], z_sem.at[1, e, p], {"ep": s},
        )

    def z_recv(s, p):
        return remote(
            send.at[s, cut(p)], rows.at[s, block(side, core, p)],
            z_sem.at[0, s, p], z_sem.at[1, s, p], {"ep": s},
        )

    def mine_copy(s, p, sems, target):
        span = rows.at[s, block(side, core, p)]
        return remote(span, span, sems.at[0, s, p], sems.at[1, s, p], {"tp": target})

    def far_copy(s, p):
        return mine_copy(s, p, far_sem, far)

    def near_copy(s, p):
        return mine_copy(s, p, near_sem, near)

    def relay_copy(s, p):
        span = rows.at[s, block(1 - side, core, p)]
        return remote(span, span, relay_sem.at[0, s, p], relay_sem.at[1, s, p], {"tp": near})

    def near_own_copy(s):
        return remote(
            part.at[s, block(side, 1 - core)], near_part.at[s, 0],
            no_sem.at[0, s], no_sem.at[1, s], {"tp": near},
        )

    def near_far_copy(s):
        return remote(
            part.at[s, block(1 - side, 1 - core)], near_part.at[s, 1],
            nf_sem.at[0, s], nf_sem.at[1, s], {"tp": near},
        )

    def far_part_copy(s, p):
        return remote(
            pair_sum.at[s, cut(p)], far_part.at[s, cut(p)],
            fp_sem.at[0, s, p], fp_sem.at[1, s, p], {"tp": far},
        )

    def return_send(s, p):
        return remote(
            result.at[s, cut(p)], returned.at[e, cut(p)],
            r_sem.at[0, s, p], r_sem.at[1, e, p], {"ep": s},
        )

    def return_recv(s, p):
        return remote(
            result.at[s, cut(p)], returned.at[s, cut(p)],
            r_sem.at[0, s, p], r_sem.at[1, s, p], {"ep": s},
        )

    state_copy = remote(
        state_out, state_in, st_sem.at[0, 0], st_sem.at[1, 0], {"ep": lax.rem(e + 1, ep)}
    )

    def memory_copy(i):
        span = memory.at[far if i == 2 else t]
        return remote(
            span, span, m_sem.at[0, i], m_sem.at[1, i], {"tp": far if i == 1 else near}
        )

    def gates(h):
        logits = logit_ref[h : h + 1, :]
        forget = (
            jnp.minimum(logits, 0.0) - jnp.log1p(jnp.exp(-jnp.abs(logits)))
        ) + extra_ref[h : h + 1, :]
        at_row = lax.broadcasted_iota(jnp.int32, (length, length), 0)
        at_col = lax.broadcasted_iota(jnp.int32, (length, length), 1)
        diagonal = at_row == at_col
        in_row = in_gate_ref[h : h + 1, :]
        in_col = jnp.sum(jnp.where(diagonal, in_row, 0.0), axis=1, keepdims=True)
        sum_col = jnp.sum(jnp.where(at_col <= at_row, forget, 0.0), axis=1, keepdims=True)
        sum_row = jnp.sum(jnp.where(diagonal, sum_col, 0.0), axis=0, keepdims=True)
        total = jnp.sum(forget, axis=1, keepdims=True)
        return in_row, in_col, sum_row, sum_col, total, at_col <= at_row

    def heads_of(ref, h):
        return ref[:, h * DH : (h + 1) * DH].astype(jnp.float32)

    def local_part():
        for h in range(heads):
            _, in_col, _, sum_col, total, _ = gates(h)
            weights = total - sum_col + in_col
            stab = jnp.max(weights, axis=0, keepdims=True)
            weighted = jnp.exp(weights - stab) * (heads_of(key_ref, h) * DH ** (-0.5))
            local_state[h, 0:DH, :] = jnp.dot(
                weighted.T, heads_of(value_ref, h), precision=highest,
                preferred_element_type=jnp.float32,
            )
            local_state[h, DH : DH + 1, :] = jnp.sum(weighted, axis=0, keepdims=True)
            local_state[h, DH + 1 : DH + 2, :] = jnp.broadcast_to(stab, (1, DH))
            local_state[h, DH + 2 : DH + 3, :] = jnp.broadcast_to(total, (1, DH))

    def pass_state():
        for h in range(heads):
            total = local_state[h, DH + 2 : DH + 3, :]
            stab_own = local_state[h, DH + 1 : DH + 2, :]
            carried = total + state_in[h, DH + 1 : DH + 2, :]
            stab = jnp.maximum(carried, stab_own)
            old, new = jnp.exp(carried - stab), jnp.exp(stab_own - stab)
            state_out[h, 0 : DH + 1, :] = (
                old * state_in[h, 0 : DH + 1, :] + new * local_state[h, 0 : DH + 1, :]
            )
            state_out[h, DH + 1 : DH + 2, :] = stab
        state_copy.start()

    def memory_part():
        for h in range(heads):
            in_row, _, sum_row, sum_col, _, causal = gates(h)
            decays = jnp.where(causal, sum_col - sum_row + in_row, -jnp.inf)
            carried_max = sum_col + state_in[h, DH + 1 : DH + 2, 0:1]
            row_max = jnp.maximum(jnp.max(decays, axis=1, keepdims=True), carried_max)
            queries = heads_of(query_ref, h)
            keys = heads_of(key_ref, h) * DH ** (-0.5)
            scores = jnp.dot(
                queries, keys.T, precision=highest, preferred_element_type=jnp.float32
            ) * jnp.exp(decays - row_max)
            carried = jnp.exp(carried_max - row_max)
            numerator = carried * jnp.dot(
                queries, state_in[h, 0:DH, :], precision=highest,
                preferred_element_type=jnp.float32,
            ) + jnp.dot(
                scores, heads_of(value_ref, h), precision=highest,
                preferred_element_type=jnp.float32,
            )
            denominator = carried * jnp.sum(
                queries * state_in[h, DH : DH + 1, :], axis=1, keepdims=True
            ) + jnp.sum(scores, axis=1, keepdims=True)
            memory[t, :, h * DH : (h + 1) * DH] = (
                numerator / jnp.maximum(jnp.abs(denominator), jnp.exp(-row_max))
            ).astype(jnp.bfloat16)
        memory_copy(0).start()
        memory_copy(1).start()

    def mix_part():
        memory_copy(1).wait_recv()
        memory_copy(2).start()
        mix_copy.wait()
        memory_copy(0).wait_recv()
        memory_copy(2).wait_recv()
        total = jnp.zeros(mixed_ref.shape, jnp.float32)
        for i in range(tp):
            total = total + jnp.dot(
                memory[i], mix[i * heads * DH : (i + 1) * heads * DH, :],
                preferred_element_type=jnp.float32,
            )
        mixed_ref[...] = total.astype(jnp.bfloat16)

    def slots():
        at_row = lax.broadcasted_iota(jnp.int32, (tok_rows, tok_rows), 0)
        at_col = lax.broadcasted_iota(jnp.int32, (tok_rows, tok_rows), 1)
        chosen = [index_ref[c : c + 1, :] == at_row for c in range(TOP)]
        member = jnp.zeros((tok_rows, tok_rows), jnp.float32)
        weights = jnp.zeros((tok_rows, tok_rows), jnp.float32)
        for c in range(TOP):
            member = member + jnp.where(chosen[c], 1.0, 0.0)
            weights = weights + jnp.where(chosen[c], weight_ref[c : c + 1, :], 0.0)
        earlier = jnp.where(at_row < at_col, 1.0, 0.0).astype(jnp.bfloat16)
        ranks = jnp.dot(member.astype(jnp.bfloat16), earlier, preferred_element_type=jnp.float32)
        slot = jnp.where(member > 0.0, ranks, -1.0)
        slot_row[...] = slot
        slot_col[...] = slot.T
        weight_col[...] = weights.T

    def norm():
        @pl.loop(0, tok_rows // GROUP)
        def _(i):
            span = pl.ds(pl.multiple_of(i * GROUP, GROUP), GROUP)
            values = tokens[span].astype(jnp.float32)
            scale = lax.rsqrt(jnp.mean(values * values, axis=1, keepdims=True) + rms_eps)
            normed[span] = (values * scale * gain_ref[...]).astype(jnp.bfloat16)

    def dispatch(x, place):
        at_slot = lax.broadcasted_iota(jnp.int32, (cap, tok_rows), 0).astype(jnp.float32)
        taken = jnp.where(at_slot == slot_row[pl.ds(x, 1), :], 1.0, 0.0).astype(jnp.bfloat16)

        @pl.loop(0, width // 512)
        def _(i):
            cols = pl.ds(pl.multiple_of(i * 512, 512), 512)
            place[:, cols] = jnp.dot(
                taken, normed[:, cols], preferred_element_type=jnp.float32
            ).astype(jnp.bfloat16)

    def combine(x, first, last):
        lane = lax.broadcasted_iota(jnp.int32, (tok_rows, tok_rows), 1)
        slot = jnp.sum(jnp.where(lane == x, slot_col[...], 0.0), axis=1, keepdims=True)
        weight = jnp.sum(jnp.where(lane == x, weight_col[...], 0.0), axis=1, keepdims=True)
        at_slot = lax.broadcasted_iota(jnp.int32, (tok_rows, cap), 1).astype(jnp.float32)
        taken = jnp.where(at_slot == slot, 1.0, 0.0).astype(jnp.bfloat16)

        @pl.loop(0, width // 512)
        def _(i):
            cols = pl.ds(pl.multiple_of(i * 512, 512), 512)
            total = weight * jnp.dot(
                taken, returned[x, :, cols], preferred_element_type=jnp.float32
            )
            if not first:
                total = total + total_out[:, cols]
            if last:
                out_ref[:, cols] = total.astype(jnp.bfloat16)
            else:
                total_out[:, cols] = total

    def feed_forward(s, group, first=False):
        span = pl.ds(pl.multiple_of(group * 2 * cap, 2 * cap), 2 * cap)
        step = 4 * LANES
        for start in range(0, 2 * part_hidden, step):
            stop = min(start + step, 2 * part_hidden)
            if first:
                for i in range(start // (2 * LANES), stop // (2 * LANES)):
                    for copy in weight_copies(i):
                        copy.wait()
            both = jnp.dot(
                rows[s, span], gate_up[:, start:stop], preferred_element_type=jnp.float32
            )
            for i in range(0, stop - start, 2 * LANES):
                act, up_act = both[:, i : i + LANES], both[:, i + LANES : i + 2 * LANES]
                at = (start + i) // 2
                hidden[:, at : at + LANES] = (jax.nn.silu(act) * up_act).astype(jnp.bfloat16)
        if first:
            down_copy.wait()
        part[s, span] = jnp.dot(
            hidden[...], down[...], preferred_element_type=jnp.float32
        ).astype(jnp.bfloat16)

    def gather_start(s, p):
        far_copy(s, p).start()
        near_copy(s, p).start()

    def land(j):
        for p in count:
            z_recv(source(j), p).wait_recv()

    def arrive(j, which=None):
        for p in count if which is None else which:
            z_recv(source(j), p).wait_recv()
            gather_start(source(j), p)

    def own_group(j, first=False):
        s = source(j)
        for p in count:
            near_copy(s, p).wait_recv()
        feed_forward(s, side, first=first)
        near_own_copy(s).start()

    def relay(j):
        s = source(j)
        for p in count:
            far_copy(s, p).wait_recv()
            relay_copy(s, p).start()

    def far_group(j):
        s = source(j)
        for p in count:
            relay_copy(s, p).wait_recv()
        feed_forward(s, 1 - side)
        near_far_copy(s).start()

    def pair(j, which=None):
        s = source(j)
        base = (1 - side) * 2 * cap + core * cap
        for p in count if which is None else which:
            if p == 0:
                near_far_copy(s).wait_recv()
            off, size = cuts[p]

            @pl.loop(0, size // GROUP)
            def _(i):
                at = pl.multiple_of(off + i * GROUP, GROUP)
                pair_sum[s, pl.ds(at, GROUP)] = (
                    part[s, pl.ds(pl.multiple_of(base + at, GROUP), GROUP)].astype(jnp.float32)
                    + near_part[s, 1, pl.ds(at, GROUP)].astype(jnp.float32)
                ).astype(jnp.bfloat16)

            far_part_copy(s, p).start()

    def finish(j, which=None, local=False):
        s = source(j)
        base = side * 2 * cap + core * cap
        for p in count if which is None else which:
            if p == 0:
                near_own_copy(s).wait_recv()
            far_part_copy(s, p).wait_recv()
            off, size = cuts[p]

            @pl.loop(0, size // GROUP)
            def _(i):
                at = pl.multiple_of(off + i * GROUP, GROUP)
                total = (
                    part[s, pl.ds(pl.multiple_of(base + at, GROUP), GROUP)].astype(jnp.float32)
                    + near_part[s, 0, pl.ds(at, GROUP)].astype(jnp.float32)
                    + far_part[s, pl.ds(at, GROUP)].astype(jnp.float32)
                ).astype(jnp.bfloat16)
                if local:
                    returned[s, pl.ds(at, GROUP)] = total
                else:
                    result[s, pl.ds(at, GROUP)] = total

            if not local:
                return_send(s, p).start()

    def gather_back(k):
        x = gathers[k]
        if k > 0:
            for p in count:
                return_recv(x, p).wait_recv()
        combine(x, k == 0, k == ep - 1)

    def start_send(k):
        for p in count:
            z_send(targets[k], p).start()

    def state_step():
        state_copy.wait_recv()

        @pl.when(e + 1 < ep)
        def _():
            pass_state()

    token_copy.start()
    for copy in head_copies:
        copy.start()

    @pl.loop(0, tiles)
    def _(i):
        for copy in weight_copies(i):
            copy.start()

    down_copy.start()
    mix_copy.start()
    barrier = pltpu.get_barrier_semaphore()

    @pl.loop(1, ep)
    def _(k):
        pl.semaphore_signal(
            barrier, inc=1, device_id={"ep": lax.rem(e + k, ep)}, device_id_type=MESH
        )

    for target in (near, far, across):
        pl.semaphore_signal(barrier, inc=1, device_id={"tp": target}, device_id_type=MESH)
    slots()
    token_copy.wait()
    norm()
    dispatch(e, rows.at[e, block(side, core)])
    pl.semaphore_wait(barrier, ep + 2)
    for p in count:
        gather_start(e, p)
    for k in range(1, ep):
        dispatch(targets[k], send.at[targets[k]])
        if k == 1 or not line:
            start_send(k)
        elif k == 2:
            pl.when(inner == 0)(functools.partial(start_send, 2))
    for copy in head_copies:
        copy.wait()
    local_part()

    @pl.when(e == 0)
    def _():
        state_in[...] = jnp.zeros_like(state_in)
        if ep > 1:
            pass_state()

    own_group(0, first=True)
    if line:
        arrive(1)
        relay(0)
        far_group(0)
        own_group(1)

        @pl.when(inner == 0)
        def _():
            arrive(2, head)
            pl.semaphore_signal(
                go_sem, inc=1, device_id={"ep": lax.rem(e + 2, ep)}, device_id_type=MESH
            )
            arrive(2, tail)

        @pl.when(inner == 1)
        def _():
            pair(0)
            pl.semaphore_wait(go_sem, 1)
            start_send(2)
            start_send(3)

        relay(1)
        far_group(1)

        @pl.when(inner == 1)
        def _():
            pair(1, head)
            arrive(2)
            pl.when(e == 1)(state_step)

        own_group(2)

        @pl.when(inner == 0)
        def _():
            pair(1)
            relay(2)
            land(3)
            start_send(3)

        @pl.when(inner == 1)
        def _():
            arrive(3, head)
            relay(2)
            arrive(3, tail)

        far_group(2)

        @pl.when(inner == 0)
        def _():
            finish(1, head)
            pair(2)
            for p in count:
                gather_start(source(3), p)
            finish(1, tail)

        own_group(3)

        @pl.when(inner == 0)
        def _():
            finish(2)
            pair(0)
            pl.when(e == ep - 1)(state_step)
            relay(3)

        @pl.when(inner == 1)
        def _():
            pair(2)
            finish(0, local=True)
            finish(1, head)
            pl.when(e == 2)(state_step)
            relay(3)

        far_group(3)

        @pl.when(inner == 0)
        def _():
            pair(3)

        @pl.when(inner == 1)
        def _():
            finish(2, head)
            pair(3)
            pair(1, tail)
            finish(2, tail)

        memory_part()

        @pl.when(inner == 0)
        def _():
            finish(0, local=True)
            finish(3)

        @pl.when(inner == 1)
        def _():
            finish(3)
            finish(1, tail)

        gather_back(0)
        gather_back(1)
        mix_part()
        gather_back(2)
        gather_back(3)
    else:
        relay(0)
        far_group(0)
        pair(0)
        finish(0, local=True)

        @pl.loop(1, ep)
        def _(j):
            arrive(j)
            own_group(j)
            relay(j)
            far_group(j)
            pl.when(e == j)(state_step)
            pair(j)
            finish(j)

        memory_part()
        mix_part()
        for k in range(ep):
            gather_back(k)

    for i in range(3):
        memory_copy(i).wait_send()

    @pl.when(e + 1 < ep)
    def _():
        state_copy.wait_send()

    @pl.loop(0, ep)
    def _(s):
        near_own_copy(s).wait_send()
        near_far_copy(s).wait_send()
        for p in count:
            far_copy(s, p).wait_send()
            near_copy(s, p).wait_send()
            relay_copy(s, p).wait_send()
            far_part_copy(s, p).wait_send()

    @pl.loop(1, ep)
    def _(k):
        s = lax.rem(e + k, ep)
        for p in count:
            z_send(s, p).wait_send()
            return_send(s, p).wait_send()


def on_device(
    memory_query_rows,
    memory_key_rows,
    memory_value_rows,
    input_gate_log,
    forget_gate_logits,
    forget_log_extra,
    memory_output_weight,
    second_batch_tokens,
    expert_norm_gain,
    routing_expert_index,
    routing_expert_weight,
    expert_gate_matrix,
    expert_up_matrix,
    expert_down_matrix,
):
    ep, tp = lax.axis_size("ep"), lax.axis_size("tp")
    tok_rows, width = second_batch_tokens.shape
    capacity = max(2, 5 * tok_rows * TOP // (4 * ep))
    cap = -(-capacity // GROUP) * GROUP
    part_hidden = expert_gate_matrix.shape[2]
    tiles = part_hidden // LANES
    positions = memory_query_rows.shape[0]
    heads = input_gate_log.shape[0]
    bf16 = jnp.bfloat16
    vmem = pl.BlockSpec(memory_space=pltpu.VMEM)
    hbm = pl.BlockSpec(memory_space=pl.ANY)
    whole = pltpu.SemaphoreType.DMA((2, ep))
    split = pltpu.SemaphoreType.DMA((2, ep, len(pieces(cap))))
    state = pltpu.VMEM((heads, DH + 8, DH), jnp.float32)
    square = pltpu.VMEM((tok_rows, tok_rows), jnp.float32)
    slotted = pltpu.VMEM((ep, cap, width), bf16)
    head_rows = pltpu.VMEM(memory_query_rows.shape, bf16)
    token_rows = pltpu.VMEM((tok_rows, width), bf16)
    return pl.pallas_call(
        functools.partial(fused_kernel, ep, tp, cap),
        out_shape=(
            jax.ShapeDtypeStruct((positions, memory_output_weight.shape[1]), bf16),
            jax.ShapeDtypeStruct((tok_rows, width), bf16),
        ),
        in_specs=[hbm] * 3 + [vmem] * 3 + [hbm] * 2 + [vmem] * 3 + [hbm] * 3,
        out_specs=(vmem, vmem),
        scratch_shapes=[
            head_rows,
            head_rows,
            head_rows,
            token_rows,
            token_rows,
            slotted,
            square,
            square,
            square,
            pltpu.VMEM((width, 2 * part_hidden), bf16),
            pltpu.VMEM((part_hidden, width), bf16),
            pltpu.VMEM((ep, tp * cap, width), bf16),
            pltpu.VMEM((2 * cap, part_hidden), bf16),
            pltpu.VMEM((ep, tp * cap, width), bf16),
            pltpu.VMEM((ep, 2, cap, width), bf16),
            slotted,
            slotted,
            slotted,
            slotted,
            pltpu.VMEM((tok_rows, width), jnp.float32),
            state,
            state,
            state,
            pltpu.VMEM((tp, positions, heads * DH), bf16),
            pltpu.VMEM(memory_output_weight.shape, bf16),
            pltpu.SemaphoreType.DMA((2, tiles)),
            pltpu.SemaphoreType.DMA((6,)),
            pltpu.SemaphoreType.DMA((2, 1)),
            split,
            split,
            split,
            split,
            whole,
            whole,
            split,
            split,
            pltpu.SemaphoreType.DMA((2, 3)),
            pltpu.SemaphoreType.REGULAR,
        ],
        compiler_params=pltpu.CompilerParams(
            collective_id=0, has_side_effects=True, vmem_limit_bytes=66000000
        ),
        cost_estimate=pl.CostEstimate(
            flops=6 * ep * tp * cap * width * part_hidden,
            bytes_accessed=6 * width * part_hidden,
            transcendentals=ep * tp * cap * part_hidden,
        ),
    )(
        memory_query_rows,
        memory_key_rows,
        memory_value_rows,
        input_gate_log,
        forget_gate_logits,
        forget_log_extra,
        memory_output_weight,
        second_batch_tokens,
        expert_norm_gain.reshape(1, -1),
        routing_expert_index.T,
        routing_expert_weight.T,
        expert_gate_matrix,
        expert_up_matrix,
        expert_down_matrix,
    )


def solution(mesh):
    placed = (
        P(("grp", "ep"), "tp"),
        P(("grp", "ep"), "tp"),
        P(("grp", "ep"), "tp"),
        P("tp", ("grp", "ep")),
        P("tp", ("grp", "ep")),
        P("tp", ("grp", "ep")),
        P(None, "tp"),
        P(("grp", "ep", "tp"), None),
        P(),
        P(("grp", "ep", "tp"), None),
        P(("grp", "ep", "tp"), None),
        P("ep", None, "tp"),
        P("ep", None, "tp"),
        P("ep", "tp", None),
    )
    return jax.shard_map(
        on_device,
        mesh=mesh,
        in_specs=placed,
        out_specs=(P(("grp", "ep"), "tp"), P(("grp", "ep", "tp"), None)),
        check_vma=False,
    )
```

```python
import functools

import jax
import jax.numpy as jnp
from jax import lax
from jax.experimental import pallas as pl
from jax.experimental.pallas import tpu as pltpu
from jax.sharding import PartitionSpec as P

DH = 128
TOP = 2

rms_eps = 1e-06
highest = lax.Precision.HIGHEST


MESH = pl.DeviceIdType.MESH
LANES = 128
GROUP = 16


def pieces(cap):
    step = cap // 32 * 16
    if step == 0:
        return [(0, cap)]
    return [(at, min(step, cap - at)) for at in range(0, cap, step)]


def fused_kernel(
    ep,
    tp,
    cap,
    query_hbm,
    key_hbm,
    value_hbm,
    in_gate_hbm,
    logit_hbm,
    extra_hbm,
    mix_hbm,
    token_hbm,
    gain_hbm,
    index_hbm,
    weight_hbm,
    gate_hbm,
    up_hbm,
    down_hbm,
    mixed_ref,
    out_ref,
    query_ref,
    key_ref,
    value_ref,
    in_gate_ref,
    logit_ref,
    extra_ref,
    gain_ref,
    index_ref,
    weight_ref,
    tokens,
    normed,
    send,
    slot_row,
    slot_col,
    weight_col,
    gate_up,
    down,
    rows,
    hidden,
    part,
    near_part,
    pair_sum,
    far_part,
    result,
    returned,
    total_out,
    local_state,
    state_in,
    state_out,
    memory,
    mix,
    w_sem,
    own_sem,
    st_sem,
    z_sem,
    far_sem,
    near_sem,
    relay_sem,
    no_sem,
    nf_sem,
    fp_sem,
    r_sem,
    m_sem,
    go_sem,
):
    e = lax.axis_index("ep")
    t = lax.axis_index("tp")
    side, core = t // 2, t % 2
    near = side * 2 + (1 - core)
    far = (1 - side) * 2 + core
    across = (1 - side) * 2 + (1 - core)
    heads = in_gate_ref.shape[0]
    length = in_gate_ref.shape[1]
    tiles = gate_up.shape[1] // (2 * LANES)
    width = rows.shape[2]
    part_hidden = down.shape[0]
    tok_rows = tokens.shape[0]
    cuts = pieces(cap)
    count = range(len(cuts))
    head, tail = count[:1], count[1:]
    line = ep == 4

    if line:
        left = 1 - e // 2
        inner = e * left + (3 - e) * (1 - left)

        def seat(v):
            return v * left + (3 - v) * (1 - left)

        targets = [e, seat(1 + 2 * inner), seat(3 - inner), seat(2 - 2 * inner)]
        sources = [e, targets[3], targets[2], targets[1]]

        def source(j):
            return sources[j]

        gathers = [e, seat(3), seat(1 + inner), seat(2 - 2 * inner)]
    else:
        targets = [lax.rem(e + k, ep) for k in range(ep)]
        gathers = targets

        def source(j):
            return lax.rem(e + ep - j, ep)

    def block(side_at, core_at, p=None):
        off, size = (0, cap) if p is None else cuts[p]
        return pl.ds(pl.multiple_of((side_at * 2 + core_at) * cap + off, GROUP), size)

    def cut(p):
        return pl.ds(cuts[p][0], cuts[p][1])

    def remote(src, dst, sent, received, target):
        return pltpu.make_async_remote_copy(
            src_ref=src,
            dst_ref=dst,
            send_sem=sent,
            recv_sem=received,
            device_id=target,
            device_id_type=MESH,
        )

    def pair_cols(i, which):
        return pl.ds(pl.multiple_of((2 * i + which) * LANES, LANES), LANES)

    def weight_copies(i):
        cols = pl.ds(pl.multiple_of(i * LANES, LANES), LANES)
        return (
            pltpu.make_async_copy(
                gate_hbm.at[0, :, cols], gate_up.at[:, pair_cols(i, 0)], w_sem.at[0, i]
            ),
            pltpu.make_async_copy(
                up_hbm.at[0, :, cols], gate_up.at[:, pair_cols(i, 1)], w_sem.at[1, i]
            ),
        )

    token_copy = pltpu.make_async_copy(token_hbm, tokens, own_sem.at[0])
    down_copy = pltpu.make_async_copy(down_hbm.at[0], down, own_sem.at[1])
    mix_copy = pltpu.make_async_copy(mix_hbm, mix, own_sem.at[2])
    head_copies = [
        pltpu.make_async_copy(query_hbm, query_ref, own_sem.at[3]),
        pltpu.make_async_copy(key_hbm, key_ref, own_sem.at[4]),
        pltpu.make_async_copy(value_hbm, value_ref, own_sem.at[5]),
        pltpu.make_async_copy(in_gate_hbm, in_gate_ref, own_sem.at[6]),
        pltpu.make_async_copy(logit_hbm, logit_ref, own_sem.at[7]),
        pltpu.make_async_copy(extra_hbm, extra_ref, own_sem.at[8]),
    ]
    route_copies = [
        pltpu.make_async_copy(index_hbm, index_ref, own_sem.at[9]),
        pltpu.make_async_copy(weight_hbm, weight_ref, own_sem.at[10]),
    ]
    gain_copy = pltpu.make_async_copy(gain_hbm, gain_ref, own_sem.at[11])

    def z_send(s, p):
        return remote(
            send.at[s, cut(p)], rows.at[e, block(side, core, p)],
            z_sem.at[0, s, p], z_sem.at[1, e, p], {"ep": s},
        )

    def z_recv(s, p):
        return remote(
            send.at[s, cut(p)], rows.at[s, block(side, core, p)],
            z_sem.at[0, s, p], z_sem.at[1, s, p], {"ep": s},
        )

    def mine_copy(s, p, sems, target):
        span = rows.at[s, block(side, core, p)]
        return remote(span, span, sems.at[0, s, p], sems.at[1, s, p], {"tp": target})

    def far_copy(s, p):
        return mine_copy(s, p, far_sem, far)

    def near_copy(s, p):
        return mine_copy(s, p, near_sem, near)

    def relay_copy(s, p):
        span = rows.at[s, block(1 - side, core, p)]
        return remote(span, span, relay_sem.at[0, s, p], relay_sem.at[1, s, p], {"tp": near})

    def near_own_copy(s):
        return remote(
            part.at[s, block(side, 1 - core)], near_part.at[s, 0],
            no_sem.at[0, s], no_sem.at[1, s], {"tp": near},
        )

    def near_far_copy(s):
        return remote(
            part.at[s, block(1 - side, 1 - core)], near_part.at[s, 1],
            nf_sem.at[0, s], nf_sem.at[1, s], {"tp": near},
        )

    def far_part_copy(s, p):
        return remote(
            pair_sum.at[s, cut(p)], far_part.at[s, cut(p)],
            fp_sem.at[0, s, p], fp_sem.at[1, s, p], {"tp": far},
        )

    def return_send(s, p):
        return remote(
            result.at[s, cut(p)], returned.at[e, cut(p)],
            r_sem.at[0, s, p], r_sem.at[1, e, p], {"ep": s},
        )

    def return_recv(s, p):
        return remote(
            result.at[s, cut(p)], returned.at[s, cut(p)],
            r_sem.at[0, s, p], r_sem.at[1, s, p], {"ep": s},
        )

    state_copy = remote(
        state_out, state_in, st_sem.at[0, 0], st_sem.at[1, 0], {"ep": lax.rem(e + 1, ep)}
    )

    def memory_copy(i):
        span = memory.at[far if i == 2 else t]
        return remote(
            span, span, m_sem.at[0, i], m_sem.at[1, i], {"tp": far if i == 1 else near}
        )

    def gates(h):
        logits = logit_ref[h : h + 1, :]
        forget = (
            jnp.minimum(logits, 0.0) - jnp.log1p(jnp.exp(-jnp.abs(logits)))
        ) + extra_ref[h : h + 1, :]
        at_row = lax.broadcasted_iota(jnp.int32, (length, length), 0)
        at_col = lax.broadcasted_iota(jnp.int32, (length, length), 1)
        diagonal = at_row == at_col
        in_row = in_gate_ref[h : h + 1, :]
        in_col = jnp.sum(jnp.where(diagonal, in_row, 0.0), axis=1, keepdims=True)
        sum_col = jnp.sum(jnp.where(at_col <= at_row, forget, 0.0), axis=1, keepdims=True)
        sum_row = jnp.sum(jnp.where(diagonal, sum_col, 0.0), axis=0, keepdims=True)
        total = jnp.sum(forget, axis=1, keepdims=True)
        return in_row, in_col, sum_row, sum_col, total, at_col <= at_row

    def heads_of(ref, h):
        return ref[:, h * DH : (h + 1) * DH].astype(jnp.float32)

    def local_part():
        for h in range(heads):
            _, in_col, _, sum_col, total, _ = gates(h)
            weights = total - sum_col + in_col
            stab = jnp.max(weights, axis=0, keepdims=True)
            weighted = jnp.exp(weights - stab) * (heads_of(key_ref, h) * DH ** (-0.5))
            local_state[h, 0:DH, :] = jnp.dot(
                weighted.T, heads_of(value_ref, h), precision=highest,
                preferred_element_type=jnp.float32,
            )
            local_state[h, DH : DH + 1, :] = jnp.sum(weighted, axis=0, keepdims=True)
            local_state[h, DH + 1 : DH + 2, :] = jnp.broadcast_to(stab, (1, DH))
            local_state[h, DH + 2 : DH + 3, :] = jnp.broadcast_to(total, (1, DH))

    def pass_state():
        for h in range(heads):
            total = local_state[h, DH + 2 : DH + 3, :]
            stab_own = local_state[h, DH + 1 : DH + 2, :]
            carried = total + state_in[h, DH + 1 : DH + 2, :]
            stab = jnp.maximum(carried, stab_own)
            old, new = jnp.exp(carried - stab), jnp.exp(stab_own - stab)
            state_out[h, 0 : DH + 1, :] = (
                old * state_in[h, 0 : DH + 1, :] + new * local_state[h, 0 : DH + 1, :]
            )
            state_out[h, DH + 1 : DH + 2, :] = stab
        state_copy.start()

    def memory_part():
        for h in range(heads):
            in_row, _, sum_row, sum_col, _, causal = gates(h)
            decays = jnp.where(causal, sum_col - sum_row + in_row, -jnp.inf)
            carried_max = sum_col + state_in[h, DH + 1 : DH + 2, 0:1]
            row_max = jnp.maximum(jnp.max(decays, axis=1, keepdims=True), carried_max)
            queries = heads_of(query_ref, h)
            keys = heads_of(key_ref, h) * DH ** (-0.5)
            scores = jnp.dot(
                queries, keys.T, precision=highest, preferred_element_type=jnp.float32
            ) * jnp.exp(decays - row_max)
            carried = jnp.exp(carried_max - row_max)
            numerator = carried * jnp.dot(
                queries, state_in[h, 0:DH, :], precision=highest,
                preferred_element_type=jnp.float32,
            ) + jnp.dot(
                scores, heads_of(value_ref, h), precision=highest,
                preferred_element_type=jnp.float32,
            )
            denominator = carried * jnp.sum(
                queries * state_in[h, DH : DH + 1, :], axis=1, keepdims=True
            ) + jnp.sum(scores, axis=1, keepdims=True)
            memory[t, :, h * DH : (h + 1) * DH] = (
                numerator / jnp.maximum(jnp.abs(denominator), jnp.exp(-row_max))
            ).astype(jnp.bfloat16)
        memory_copy(0).start()
        memory_copy(1).start()

    def memory_relay():
        memory_copy(1).wait_recv()
        memory_copy(2).start()

    def mix_part():
        mix_copy.wait()
        memory_copy(0).wait_recv()
        memory_copy(2).wait_recv()
        total = jnp.zeros(mixed_ref.shape, jnp.float32)
        for i in range(tp):
            total = total + jnp.dot(
                memory[i], mix[i * heads * DH : (i + 1) * heads * DH, :],
                preferred_element_type=jnp.float32,
            )
        mixed_ref[...] = total.astype(jnp.bfloat16)

    def slots():
        at_row = lax.broadcasted_iota(jnp.int32, (tok_rows, tok_rows), 0)
        at_col = lax.broadcasted_iota(jnp.int32, (tok_rows, tok_rows), 1)
        chosen = [index_ref[c : c + 1, :] == at_row for c in range(TOP)]
        member = jnp.zeros((tok_rows, tok_rows), jnp.float32)
        weights = jnp.zeros((tok_rows, tok_rows), jnp.float32)
        for c in range(TOP):
            member = member + jnp.where(chosen[c], 1.0, 0.0)
            weights = weights + jnp.where(chosen[c], weight_ref[c : c + 1, :], 0.0)
        earlier = jnp.where(at_row < at_col, 1.0, 0.0).astype(jnp.bfloat16)
        ranks = jnp.dot(member.astype(jnp.bfloat16), earlier, preferred_element_type=jnp.float32)
        slot = jnp.where(member > 0.0, ranks, -1.0)
        slot_row[...] = slot
        slot_col[...] = slot.T
        weight_col[...] = weights.T

    def norm():
        @pl.loop(0, tok_rows // GROUP)
        def _(i):
            span = pl.ds(pl.multiple_of(i * GROUP, GROUP), GROUP)
            values = tokens[span].astype(jnp.float32)
            scale = lax.rsqrt(jnp.mean(values * values, axis=1, keepdims=True) + rms_eps)
            normed[span] = (values * scale * gain_ref[...]).astype(jnp.bfloat16)

    def dispatch(x, place):
        at_slot = lax.broadcasted_iota(jnp.int32, (cap, tok_rows), 0).astype(jnp.float32)
        taken = jnp.where(at_slot == slot_row[pl.ds(x, 1), :], 1.0, 0.0).astype(jnp.bfloat16)

        place[...] = jnp.dot(
            taken, normed[...], preferred_element_type=jnp.float32
        ).astype(jnp.bfloat16)

    def combine(x, first, last):
        lane = lax.broadcasted_iota(jnp.int32, (tok_rows, tok_rows), 1)
        slot = jnp.sum(jnp.where(lane == x, slot_col[...], 0.0), axis=1, keepdims=True)
        weight = jnp.sum(jnp.where(lane == x, weight_col[...], 0.0), axis=1, keepdims=True)
        at_slot = lax.broadcasted_iota(jnp.int32, (tok_rows, cap), 1).astype(jnp.float32)
        taken = jnp.where(at_slot == slot, 1.0, 0.0).astype(jnp.bfloat16)

        total = weight * jnp.dot(taken, returned[x], preferred_element_type=jnp.float32)
        if not first:
            total = total + total_out[...]
        if last:
            out_ref[...] = total.astype(jnp.bfloat16)
        else:
            total_out[...] = total

    def feed_forward(s, group, first=False):
        span = pl.ds(pl.multiple_of(group * 2 * cap, 2 * cap), 2 * cap)
        step = 4 * LANES
        for start in range(0, 2 * part_hidden, step):
            stop = min(start + step, 2 * part_hidden)
            if first:
                for i in range(start // (2 * LANES), stop // (2 * LANES)):
                    for copy in weight_copies(i):
                        copy.wait()
            both = jnp.dot(
                rows[s, span], gate_up[:, start:stop], preferred_element_type=jnp.float32
            )
            for i in range(0, stop - start, 2 * LANES):
                act, up_act = both[:, i : i + LANES], both[:, i + LANES : i + 2 * LANES]
                at = (start + i) // 2
                hidden[:, at : at + LANES] = (jax.nn.silu(act) * up_act).astype(jnp.bfloat16)
        if first:
            down_copy.wait()
        part[s, span] = jnp.dot(
            hidden[...], down[...], preferred_element_type=jnp.float32
        ).astype(jnp.bfloat16)

    def gather_start(s, p):
        far_copy(s, p).start()
        near_copy(s, p).start()

    def land(j):
        for p in count:
            z_recv(source(j), p).wait_recv()

    def arrive(j, which=None):
        for p in count if which is None else which:
            z_recv(source(j), p).wait_recv()
            gather_start(source(j), p)

    def own_group(j, first=False):
        s = source(j)
        for p in count:
            near_copy(s, p).wait_recv()
        feed_forward(s, side, first=first)
        near_own_copy(s).start()

    def relay(j):
        s = source(j)
        for p in count:
            far_copy(s, p).wait_recv()
            relay_copy(s, p).start()

    def far_group(j):
        s = source(j)
        for p in count:
            relay_copy(s, p).wait_recv()
        feed_forward(s, 1 - side)
        near_far_copy(s).start()

    def pair(j, which=None):
        s = source(j)
        base = (1 - side) * 2 * cap + core * cap
        for p in count if which is None else which:
            if p == 0:
                near_far_copy(s).wait_recv()
            off, size = cuts[p]

            @pl.loop(0, size // GROUP)
            def _(i):
                at = pl.multiple_of(off + i * GROUP, GROUP)
                pair_sum[s, pl.ds(at, GROUP)] = (
                    part[s, pl.ds(pl.multiple_of(base + at, GROUP), GROUP)].astype(jnp.float32)
                    + near_part[s, 1, pl.ds(at, GROUP)].astype(jnp.float32)
                ).astype(jnp.bfloat16)

            far_part_copy(s, p).start()

    def finish(j, which=None, local=False):
        s = source(j)
        base = side * 2 * cap + core * cap
        for p in count if which is None else which:
            if p == 0:
                near_own_copy(s).wait_recv()
            far_part_copy(s, p).wait_recv()
            off, size = cuts[p]

            @pl.loop(0, size // GROUP)
            def _(i):
                at = pl.multiple_of(off + i * GROUP, GROUP)
                total = (
                    part[s, pl.ds(pl.multiple_of(base + at, GROUP), GROUP)].astype(jnp.float32)
                    + near_part[s, 0, pl.ds(at, GROUP)].astype(jnp.float32)
                    + far_part[s, pl.ds(at, GROUP)].astype(jnp.float32)
                ).astype(jnp.bfloat16)
                if local:
                    returned[s, pl.ds(at, GROUP)] = total
                else:
                    result[s, pl.ds(at, GROUP)] = total

            if not local:
                return_send(s, p).start()

    def gather_back(k, first=False, last=False):
        x = gathers[k]
        if k > 0:
            for p in count:
                return_recv(x, p).wait_recv()
        combine(x, first, last)

    def start_send(k):
        for p in count:
            z_send(targets[k], p).start()

    def drain():
        for i in range(3):
            memory_copy(i).wait_send()

        @pl.when(e + 1 < ep)
        def _():
            state_copy.wait_send()

        @pl.loop(0, ep)
        def _(s):
            near_own_copy(s).wait_send()
            near_far_copy(s).wait_send()
            for p in count:
                far_copy(s, p).wait_send()
                near_copy(s, p).wait_send()
                relay_copy(s, p).wait_send()
                far_part_copy(s, p).wait_send()

        @pl.loop(1, ep)
        def _(k):
            s = lax.rem(e + k, ep)
            for p in count:
                z_send(s, p).wait_send()
                return_send(s, p).wait_send()

    def state_step():
        state_copy.wait_recv()

        @pl.when(e + 1 < ep)
        def _():
            pass_state()

    for copy in route_copies:
        copy.start()
    token_copy.start()
    gain_copy.start()
    for copy in head_copies:
        copy.start()

    @pl.loop(0, tiles)
    def _(i):
        for copy in weight_copies(i):
            copy.start()

    down_copy.start()
    mix_copy.start()
    barrier = pltpu.get_barrier_semaphore()

    @pl.loop(1, ep)
    def _(k):
        pl.semaphore_signal(
            barrier, inc=1, device_id={"ep": lax.rem(e + k, ep)}, device_id_type=MESH
        )

    for target in (near, far, across):
        pl.semaphore_signal(barrier, inc=1, device_id={"tp": target}, device_id_type=MESH)
    for copy in route_copies:
        copy.wait()
    slots()
    gain_copy.wait()
    token_copy.wait()
    norm()
    dispatch(e, rows.at[e, block(side, core)])
    pl.semaphore_wait(barrier, ep + 2)
    for p in count:
        gather_start(e, p)
    for k in range(1, ep):
        dispatch(targets[k], send.at[targets[k]])
        if k == 1 or not line:
            start_send(k)
        elif k == 2:
            pl.when(inner == 0)(functools.partial(start_send, 2))
    for copy in head_copies:
        copy.wait()
    local_part()

    @pl.when(e == 0)
    def _():
        state_in[...] = jnp.zeros_like(state_in)
        if ep > 1:
            pass_state()

    own_group(0, first=True)
    if line:
        arrive(1)
        relay(0)
        far_group(0)
        own_group(1)

        @pl.when(inner == 0)
        def _():
            arrive(2, head)
            pl.semaphore_signal(
                go_sem, inc=1, device_id={"ep": lax.rem(e + 2, ep)}, device_id_type=MESH
            )
            arrive(2, tail)

        @pl.when(inner == 1)
        def _():
            pair(0, count[:-1])
            pl.semaphore_wait(go_sem, 1)
            start_send(2)
            start_send(3)

        relay(1)
        far_group(1)

        @pl.when(inner == 1)
        def _():
            pair(1)
            pl.when(e == 1)(state_step)
            arrive(2)

        own_group(2)

        @pl.when(inner == 0)
        def _():
            pair(1)
            relay(2)
            land(3)
            pl.when(e > 0)(functools.partial(start_send, 3))

        @pl.when(inner == 1)
        def _():
            pl.when(e == 2)(state_step)
            arrive(3, head)
            relay(2)
            arrive(3, tail)

        far_group(2)

        @pl.when(inner == 0)
        def _():
            pl.when(e == 0)(functools.partial(start_send, 3))
            finish(1, head)
            pair(2)
            for p in count:
                gather_start(source(3), p)
            finish(1, tail)

        own_group(3)

        @pl.when(inner == 0)
        def _():
            finish(2)
            pair(0)
            pl.when(e > 0)(state_step)

        @pl.when(inner == 1)
        def _():
            pair(2)
            finish(1)
            finish(0, count[:-1], local=True)

        memory_part()
        relay(3)
        far_group(3)

        @pl.when(inner == 0)
        def _():
            pair(3)
            memory_relay()
            finish(0, local=True)

        @pl.when(inner == 1)
        def _():
            finish(2, head)
            pair(3)
            memory_relay()
            pair(0, count[-1:])
            finish(2, tail)

        gather_back(1, first=True)
        finish(3, head)
        mix_part()
        finish(3, tail)

        @pl.when(inner == 1)
        def _():
            finish(0, count[-1:], local=True)

        gather_back(0)
        gather_back(2)
        drain()
        gather_back(3, last=True)
    else:
        relay(0)
        far_group(0)
        pair(0)
        finish(0, local=True)

        @pl.loop(1, ep)
        def _(j):
            arrive(j)
            own_group(j)
            relay(j)
            far_group(j)
            pl.when(e == j)(state_step)
            pair(j)
            finish(j)

        memory_part()
        memory_relay()
        mix_part()
        for k in range(ep):
            gather_back(k, k == 0, k == ep - 1)
        drain()


def on_device(
    memory_query_rows,
    memory_key_rows,
    memory_value_rows,
    input_gate_log,
    forget_gate_logits,
    forget_log_extra,
    memory_output_weight,
    second_batch_tokens,
    expert_norm_gain,
    routing_expert_index,
    routing_expert_weight,
    expert_gate_matrix,
    expert_up_matrix,
    expert_down_matrix,
):
    ep, tp = lax.axis_size("ep"), lax.axis_size("tp")
    tok_rows, width = second_batch_tokens.shape
    capacity = max(2, 5 * tok_rows * TOP // (4 * ep))
    cap = -(-capacity // GROUP) * GROUP
    part_hidden = expert_gate_matrix.shape[2]
    tiles = part_hidden // LANES
    positions = memory_query_rows.shape[0]
    heads = input_gate_log.shape[0]
    bf16 = jnp.bfloat16
    vmem = pl.BlockSpec(memory_space=pltpu.VMEM)
    hbm = pl.BlockSpec(memory_space=pl.ANY)
    whole = pltpu.SemaphoreType.DMA((2, ep))
    split = pltpu.SemaphoreType.DMA((2, ep, len(pieces(cap))))
    state = pltpu.VMEM((heads, DH + 8, DH), jnp.float32)
    square = pltpu.VMEM((tok_rows, tok_rows), jnp.float32)
    slotted = pltpu.VMEM((ep, cap, width), bf16)
    head_rows = pltpu.VMEM(memory_query_rows.shape, bf16)
    token_rows = pltpu.VMEM((tok_rows, width), bf16)
    head_gates = pltpu.VMEM(input_gate_log.shape, jnp.float32)
    return pl.pallas_call(
        functools.partial(fused_kernel, ep, tp, cap),
        out_shape=(
            pltpu.VMEM((positions, memory_output_weight.shape[1]), bf16),
            pltpu.VMEM((tok_rows, width), bf16),
        ),
        in_specs=[hbm] * 14,
        out_specs=(vmem, vmem),
        scratch_shapes=[
            head_rows,
            head_rows,
            head_rows,
            head_gates,
            head_gates,
            head_gates,
            pltpu.VMEM((1, width), jnp.float32),
            pltpu.VMEM((TOP, tok_rows), jnp.int32),
            pltpu.VMEM((TOP, tok_rows), jnp.float32),
            token_rows,
            token_rows,
            slotted,
            square,
            square,
            square,
            pltpu.VMEM((width, 2 * part_hidden), bf16),
            pltpu.VMEM((part_hidden, width), bf16),
            pltpu.VMEM((ep, tp * cap, width), bf16),
            pltpu.VMEM((2 * cap, part_hidden), bf16),
            pltpu.VMEM((ep, tp * cap, width), bf16),
            pltpu.VMEM((ep, 2, cap, width), bf16),
            slotted,
            slotted,
            slotted,
            slotted,
            pltpu.VMEM((tok_rows, width), jnp.float32),
            state,
            state,
            state,
            pltpu.VMEM((tp, positions, heads * DH), bf16),
            pltpu.VMEM(memory_output_weight.shape, bf16),
            pltpu.SemaphoreType.DMA((2, tiles)),
            pltpu.SemaphoreType.DMA((12,)),
            pltpu.SemaphoreType.DMA((2, 1)),
            split,
            split,
            split,
            split,
            whole,
            whole,
            split,
            split,
            pltpu.SemaphoreType.DMA((2, 3)),
            pltpu.SemaphoreType.REGULAR,
        ],
        compiler_params=pltpu.CompilerParams(
            collective_id=0, has_side_effects=True, vmem_limit_bytes=66000000
        ),
        cost_estimate=pl.CostEstimate(
            flops=6 * ep * tp * cap * width * part_hidden,
            bytes_accessed=6 * width * part_hidden,
            transcendentals=ep * tp * cap * part_hidden,
        ),
    )(
        memory_query_rows,
        memory_key_rows,
        memory_value_rows,
        input_gate_log,
        forget_gate_logits,
        forget_log_extra,
        memory_output_weight,
        second_batch_tokens,
        expert_norm_gain.reshape(1, -1),
        routing_expert_index.T,
        routing_expert_weight.T,
        expert_gate_matrix,
        expert_up_matrix,
        expert_down_matrix,
    )


def solution(mesh):
    placed = (
        P(("grp", "ep"), "tp"),
        P(("grp", "ep"), "tp"),
        P(("grp", "ep"), "tp"),
        P("tp", ("grp", "ep")),
        P("tp", ("grp", "ep")),
        P("tp", ("grp", "ep")),
        P(None, "tp"),
        P(("grp", "ep", "tp"), None),
        P(),
        P(("grp", "ep", "tp"), None),
        P(("grp", "ep", "tp"), None),
        P("ep", None, "tp"),
        P("ep", None, "tp"),
        P("ep", "tp", None),
    )
    return jax.shard_map(
        on_device,
        mesh=mesh,
        in_specs=placed,
        out_specs=(P(("grp", "ep"), "tp"), P(("grp", "ep", "tp"), None)),
        check_vma=False,
    )
```

```python
import functools

import jax
import jax.numpy as jnp
from jax import lax
from jax.experimental import pallas as pl
from jax.experimental.pallas import tpu as pltpu
from jax.sharding import PartitionSpec as P

DH = 128
TOP = 2

rms_eps = 1e-06
highest = lax.Precision.HIGHEST


MESH = pl.DeviceIdType.MESH
LANES = 128
GROUP = 16


def pieces(cap):
    step = cap // 32 * 16
    if step == 0:
        return [(0, cap)]
    return [(at, min(step, cap - at)) for at in range(0, cap, step)]


def fused_kernel(
    ep,
    tp,
    cap,
    query_hbm,
    key_hbm,
    value_hbm,
    in_gate_hbm,
    logit_hbm,
    extra_hbm,
    mix_hbm,
    token_hbm,
    gain_hbm,
    index_hbm,
    weight_hbm,
    gate_hbm,
    up_hbm,
    down_hbm,
    mixed_ref,
    out_ref,
    query_ref,
    key_ref,
    value_ref,
    in_gate_ref,
    logit_ref,
    extra_ref,
    gain_ref,
    index_ref,
    weight_ref,
    tokens,
    normed,
    send,
    slot_row,
    slot_col,
    weight_col,
    gate_up,
    down,
    rows,
    hidden,
    part,
    near_part,
    pair_sum,
    far_part,
    result,
    returned,
    total_out,
    local_state,
    state_in,
    state_out,
    memory,
    mix,
    w_sem,
    own_sem,
    st_sem,
    sent_sem,
    z_sem,
    far_sem,
    near_sem,
    relay_sem,
    no_sem,
    nf_sem,
    fp_sem,
    r_sem,
    m_sem,
):
    e = lax.axis_index("ep")
    t = lax.axis_index("tp")
    side, core = t // 2, t % 2
    near = side * 2 + (1 - core)
    far = (1 - side) * 2 + core
    across = (1 - side) * 2 + (1 - core)
    heads = in_gate_ref.shape[0]
    length = in_gate_ref.shape[1]
    tiles = gate_up.shape[1] // (2 * LANES)
    width = rows.shape[2]
    part_hidden = down.shape[0]
    tok_rows = tokens.shape[0]
    cuts = pieces(cap)
    count = range(len(cuts))
    head, tail = count[:1], count[1:]
    most, last = count[:-1], count[-1:]
    line = ep == 4

    if line:
        left = 1 - e // 2
        inner = e * left + (3 - e) * (1 - left)

        def seat(v):
            return v * left + (3 - v) * (1 - left)

        targets = [e, seat(1 + 2 * inner), seat(3 - inner), seat(2 - 2 * inner)]
        sources = [e, seat(2 - 2 * inner), seat(1 + inner), seat(3)]

        def source(j):
            return sources[j]

        gathers = [e, seat(1 + 2 * inner), seat(3 - inner), seat(2 - 2 * inner)]
    else:
        targets = [lax.rem(e + k, ep) for k in range(ep)]
        gathers = targets

        def source(j):
            return lax.rem(e + ep - j, ep)

    def block(side_at, core_at, p=None):
        off, size = (0, cap) if p is None else cuts[p]
        return pl.ds(pl.multiple_of((side_at * 2 + core_at) * cap + off, GROUP), size)

    def cut(p):
        return pl.ds(cuts[p][0], cuts[p][1])

    def remote(src, dst, sent, received, target):
        return pltpu.make_async_remote_copy(
            src_ref=src,
            dst_ref=dst,
            send_sem=sent,
            recv_sem=received,
            device_id=target,
            device_id_type=MESH,
        )

    def pair_cols(i, which):
        return pl.ds(pl.multiple_of((2 * i + which) * LANES, LANES), LANES)

    def weight_copies(i):
        cols = pl.ds(pl.multiple_of(i * LANES, LANES), LANES)
        return (
            pltpu.make_async_copy(
                gate_hbm.at[0, :, cols], gate_up.at[:, pair_cols(i, 0)], w_sem.at[0, i]
            ),
            pltpu.make_async_copy(
                up_hbm.at[0, :, cols], gate_up.at[:, pair_cols(i, 1)], w_sem.at[1, i]
            ),
        )

    token_copy = pltpu.make_async_copy(token_hbm, tokens, own_sem.at[0])
    down_copy = pltpu.make_async_copy(down_hbm.at[0], down, own_sem.at[1])
    mix_copy = pltpu.make_async_copy(mix_hbm, mix, own_sem.at[2])
    head_copies = [
        pltpu.make_async_copy(query_hbm, query_ref, own_sem.at[3]),
        pltpu.make_async_copy(key_hbm, key_ref, own_sem.at[4]),
        pltpu.make_async_copy(value_hbm, value_ref, own_sem.at[5]),
        pltpu.make_async_copy(in_gate_hbm, in_gate_ref, own_sem.at[6]),
        pltpu.make_async_copy(logit_hbm, logit_ref, own_sem.at[7]),
        pltpu.make_async_copy(extra_hbm, extra_ref, own_sem.at[8]),
    ]
    route_copies = [
        pltpu.make_async_copy(index_hbm, index_ref, own_sem.at[9]),
        pltpu.make_async_copy(weight_hbm, weight_ref, own_sem.at[10]),
    ]
    gain_copy = pltpu.make_async_copy(gain_hbm, gain_ref, own_sem.at[11])

    def z_send(s, p):
        return remote(
            send.at[s, cut(p)], rows.at[e, block(side, core, p)],
            sent_sem.at[0], z_sem.at[e, p], {"ep": s},
        )

    def z_recv(s, p):
        return remote(
            send.at[s, cut(p)], rows.at[s, block(side, core, p)],
            sent_sem.at[0], z_sem.at[s, p], {"ep": s},
        )

    def far_copy(s, p):
        span = rows.at[s, block(side, core, p)]
        return remote(span, span, sent_sem.at[1], far_sem.at[s, p], {"tp": far})

    def near_copy(s, p):
        span = rows.at[s, block(side, core, p)]
        return remote(span, span, sent_sem.at[2], near_sem.at[s, p], {"tp": near})

    def relay_copy(s, p):
        span = rows.at[s, block(1 - side, core, p)]
        return remote(span, span, sent_sem.at[3], relay_sem.at[s, p], {"tp": near})

    def near_own_copy(s):
        return remote(
            part.at[s, block(side, 1 - core)], near_part.at[s, 0],
            sent_sem.at[4], no_sem.at[s], {"tp": near},
        )

    def near_far_copy(s):
        return remote(
            part.at[s, block(1 - side, 1 - core)], near_part.at[s, 1],
            sent_sem.at[5], nf_sem.at[s], {"tp": near},
        )

    def far_part_copy(s, p):
        return remote(
            pair_sum.at[s, cut(p)], far_part.at[s, cut(p)],
            sent_sem.at[6], fp_sem.at[s, p], {"tp": far},
        )

    def return_send(s, p):
        return remote(
            result.at[s, cut(p)], returned.at[e, cut(p)],
            sent_sem.at[7], r_sem.at[e, p], {"ep": s},
        )

    def return_recv(s, p):
        return remote(
            result.at[s, cut(p)], returned.at[s, cut(p)],
            sent_sem.at[7], r_sem.at[s, p], {"ep": s},
        )

    state_copy = remote(
        state_out, state_in, st_sem.at[0, 0], st_sem.at[1, 0], {"ep": lax.rem(e + 1, ep)}
    )

    def memory_copy(i):
        span = memory.at[far if i == 2 else t]
        return remote(
            span, span, m_sem.at[0, i], m_sem.at[1, i], {"tp": far if i == 1 else near}
        )

    def gates(h):
        logits = logit_ref[h : h + 1, :]
        forget = (
            jnp.minimum(logits, 0.0) - jnp.log1p(jnp.exp(-jnp.abs(logits)))
        ) + extra_ref[h : h + 1, :]
        at_row = lax.broadcasted_iota(jnp.int32, (length, length), 0)
        at_col = lax.broadcasted_iota(jnp.int32, (length, length), 1)
        diagonal = at_row == at_col
        in_row = in_gate_ref[h : h + 1, :]
        in_col = jnp.sum(jnp.where(diagonal, in_row, 0.0), axis=1, keepdims=True)
        sum_col = jnp.sum(jnp.where(at_col <= at_row, forget, 0.0), axis=1, keepdims=True)
        sum_row = jnp.sum(jnp.where(diagonal, sum_col, 0.0), axis=0, keepdims=True)
        total = jnp.sum(forget, axis=1, keepdims=True)
        return in_row, in_col, sum_row, sum_col, total, at_col <= at_row

    def heads_of(ref, h):
        return ref[:, h * DH : (h + 1) * DH].astype(jnp.float32)

    def local_part():
        for h in range(heads):
            _, in_col, _, sum_col, total, _ = gates(h)
            weights = total - sum_col + in_col
            stab = jnp.max(weights, axis=0, keepdims=True)
            weighted = jnp.exp(weights - stab) * (heads_of(key_ref, h) * DH ** (-0.5))
            local_state[h, 0:DH, :] = jnp.dot(
                weighted.T, heads_of(value_ref, h), precision=highest,
                preferred_element_type=jnp.float32,
            )
            local_state[h, DH : DH + 1, :] = jnp.sum(weighted, axis=0, keepdims=True)
            local_state[h, DH + 1 : DH + 2, :] = jnp.broadcast_to(stab, (1, DH))
            local_state[h, DH + 2 : DH + 3, :] = jnp.broadcast_to(total, (1, DH))

    def pass_state():
        for h in range(heads):
            total = local_state[h, DH + 2 : DH + 3, :]
            stab_own = local_state[h, DH + 1 : DH + 2, :]
            carried = total + state_in[h, DH + 1 : DH + 2, :]
            stab = jnp.maximum(carried, stab_own)
            old, new = jnp.exp(carried - stab), jnp.exp(stab_own - stab)
            state_out[h, 0 : DH + 1, :] = (
                old * state_in[h, 0 : DH + 1, :] + new * local_state[h, 0 : DH + 1, :]
            )
            state_out[h, DH + 1 : DH + 2, :] = stab
        state_copy.start()

    def memory_part():
        for h in range(heads):
            in_row, _, sum_row, sum_col, _, causal = gates(h)
            decays = jnp.where(causal, sum_col - sum_row + in_row, -jnp.inf)
            carried_max = sum_col + state_in[h, DH + 1 : DH + 2, 0:1]
            row_max = jnp.maximum(jnp.max(decays, axis=1, keepdims=True), carried_max)
            queries = heads_of(query_ref, h)
            keys = heads_of(key_ref, h) * DH ** (-0.5)
            scores = jnp.dot(
                queries, keys.T, precision=highest, preferred_element_type=jnp.float32
            ) * jnp.exp(decays - row_max)
            carried = jnp.exp(carried_max - row_max)
            numerator = carried * jnp.dot(
                queries, state_in[h, 0:DH, :], precision=highest,
                preferred_element_type=jnp.float32,
            ) + jnp.dot(
                scores, heads_of(value_ref, h), precision=highest,
                preferred_element_type=jnp.float32,
            )
            denominator = carried * jnp.sum(
                queries * state_in[h, DH : DH + 1, :], axis=1, keepdims=True
            ) + jnp.sum(scores, axis=1, keepdims=True)
            memory[t, :, h * DH : (h + 1) * DH] = (
                numerator / jnp.maximum(jnp.abs(denominator), jnp.exp(-row_max))
            ).astype(jnp.bfloat16)
        memory_copy(0).start()
        memory_copy(1).start()

    def memory_relay():
        memory_copy(1).wait_recv()
        memory_copy(2).start()

    def mix_part():
        mix_copy.wait()
        memory_copy(0).wait_recv()
        memory_copy(2).wait_recv()
        total = jnp.zeros(mixed_ref.shape, jnp.float32)
        for i in range(tp):
            total = total + jnp.dot(
                memory[i], mix[i * heads * DH : (i + 1) * heads * DH, :],
                preferred_element_type=jnp.float32,
            )
        mixed_ref[...] = total.astype(jnp.bfloat16)

    def slots():
        at_row = lax.broadcasted_iota(jnp.int32, (tok_rows, tok_rows), 0)
        at_col = lax.broadcasted_iota(jnp.int32, (tok_rows, tok_rows), 1)
        chosen = [index_ref[c : c + 1, :] == at_row for c in range(TOP)]
        member = jnp.zeros((tok_rows, tok_rows), jnp.float32)
        weights = jnp.zeros((tok_rows, tok_rows), jnp.float32)
        for c in range(TOP):
            member = member + jnp.where(chosen[c], 1.0, 0.0)
            weights = weights + jnp.where(chosen[c], weight_ref[c : c + 1, :], 0.0)
        earlier = jnp.where(at_row < at_col, 1.0, 0.0).astype(jnp.bfloat16)
        ranks = jnp.dot(member.astype(jnp.bfloat16), earlier, preferred_element_type=jnp.float32)
        slot = jnp.where(member > 0.0, ranks, -1.0)
        slot_row[...] = slot
        slot_col[...] = slot.T
        weight_col[...] = weights.T

    def norm():
        @pl.loop(0, tok_rows // GROUP, unroll=4)
        def _(i):
            span = pl.ds(pl.multiple_of(i * GROUP, GROUP), GROUP)
            values = tokens[span].astype(jnp.float32)
            scale = lax.rsqrt(jnp.mean(values * values, axis=1, keepdims=True) + rms_eps)
            normed[span] = (values * scale * gain_ref[...]).astype(jnp.bfloat16)

    def dispatch(x, place):
        at_slot = lax.broadcasted_iota(jnp.int32, (cap, tok_rows), 0).astype(jnp.float32)
        taken = jnp.where(at_slot == slot_row[pl.ds(x, 1), :], 1.0, 0.0).astype(jnp.bfloat16)

        place[...] = jnp.dot(
            taken, normed[...], preferred_element_type=jnp.float32
        ).astype(jnp.bfloat16)

    def combine(x, first, last):
        lane = lax.broadcasted_iota(jnp.int32, (tok_rows, tok_rows), 1)
        slot = jnp.sum(jnp.where(lane == x, slot_col[...], 0.0), axis=1, keepdims=True)
        weight = jnp.sum(jnp.where(lane == x, weight_col[...], 0.0), axis=1, keepdims=True)
        at_slot = lax.broadcasted_iota(jnp.int32, (tok_rows, cap), 1).astype(jnp.float32)
        taken = jnp.where(at_slot == slot, 1.0, 0.0).astype(jnp.bfloat16)

        total = weight * jnp.dot(taken, returned[x], preferred_element_type=jnp.float32)
        if not first:
            total = total + total_out[...]
        if last:
            out_ref[...] = total.astype(jnp.bfloat16)
        else:
            total_out[...] = total

    def feed_forward(s, group, first=False):
        span = pl.ds(pl.multiple_of(group * 2 * cap, 2 * cap), 2 * cap)
        step = 4 * LANES
        for start in range(0, 2 * part_hidden, step):
            stop = min(start + step, 2 * part_hidden)
            if first:
                for i in range(start // (2 * LANES), stop // (2 * LANES)):
                    for copy in weight_copies(i):
                        copy.wait()
            both = jnp.dot(
                rows[s, span], gate_up[:, start:stop], preferred_element_type=jnp.float32
            )
            for i in range(0, stop - start, 2 * LANES):
                act, up_act = both[:, i : i + LANES], both[:, i + LANES : i + 2 * LANES]
                at = (start + i) // 2
                hidden[:, at : at + LANES] = (jax.nn.silu(act) * up_act).astype(jnp.bfloat16)
        if first:
            down_copy.wait()
        part[s, span] = jnp.dot(
            hidden[...], down[...], preferred_element_type=jnp.float32
        ).astype(jnp.bfloat16)

    def gather_start(s, p):
        far_copy(s, p).start()
        near_copy(s, p).start()

    def arrive(j, which=None):
        for p in count if which is None else which:
            z_recv(source(j), p).wait_recv()
            gather_start(source(j), p)

    def weave(j, k):
        for p in most:
            arrive(j, [p])
            relay(k, [p])
        relay(k, last)
        arrive(j, last)

    def own_group(j, first=False):
        s = source(j)
        for p in count:
            near_copy(s, p).wait_recv()
        feed_forward(s, side, first=first)
        near_own_copy(s).start()

    def relay(j, which=None):
        s = source(j)
        for p in count if which is None else which:
            far_copy(s, p).wait_recv()
            relay_copy(s, p).start()

    def far_group(j):
        s = source(j)
        for p in count:
            relay_copy(s, p).wait_recv()
        feed_forward(s, 1 - side)
        near_far_copy(s).start()

    def pair(j, which=None):
        s = source(j)
        base = (1 - side) * 2 * cap + core * cap
        for p in count if which is None else which:
            if p == 0:
                near_far_copy(s).wait_recv()
            off, size = cuts[p]

            @pl.loop(0, size // GROUP)
            def _(i):
                at = pl.multiple_of(off + i * GROUP, GROUP)
                pair_sum[s, pl.ds(at, GROUP)] = (
                    part[s, pl.ds(pl.multiple_of(base + at, GROUP), GROUP)].astype(jnp.float32)
                    + near_part[s, 1, pl.ds(at, GROUP)].astype(jnp.float32)
                ).astype(jnp.bfloat16)

            far_part_copy(s, p).start()

    def finish(j, which=None, local=False):
        s = source(j)
        base = side * 2 * cap + core * cap
        for p in count if which is None else which:
            if p == 0:
                near_own_copy(s).wait_recv()
            far_part_copy(s, p).wait_recv()
            off, size = cuts[p]

            @pl.loop(0, size // GROUP)
            def _(i):
                at = pl.multiple_of(off + i * GROUP, GROUP)
                total = (
                    part[s, pl.ds(pl.multiple_of(base + at, GROUP), GROUP)].astype(jnp.float32)
                    + near_part[s, 0, pl.ds(at, GROUP)].astype(jnp.float32)
                    + far_part[s, pl.ds(at, GROUP)].astype(jnp.float32)
                ).astype(jnp.bfloat16)
                if local:
                    returned[s, pl.ds(at, GROUP)] = total
                else:
                    result[s, pl.ds(at, GROUP)] = total

            if not local:
                return_send(s, p).start()

    def gather_back(k, first=False, last=False):
        x = gathers[k]
        if k > 0:
            for p in count:
                return_recv(x, p).wait_recv()
        combine(x, first, last)

    def start_send(k):
        for p in count:
            z_send(targets[k], p).start()

    def drain():
        for i in range(3):
            memory_copy(i).wait_send()

        @pl.when(e + 1 < ep)
        def _():
            state_copy.wait_send()

        for k in range(8):
            stages = ep - 1 if k in (0, 7) else ep
            if stages:
                span = send.at[pl.ds(0, stages)]
                remote(
                    span, span, sent_sem.at[k], no_sem.at[0], {"tp": near}
                ).wait_send()

    def state_step():
        state_copy.wait_recv()

        @pl.when(e + 1 < ep)
        def _():
            pass_state()

    for copy in route_copies:
        copy.start()
    token_copy.start()
    gain_copy.start()
    for copy in head_copies:
        copy.start()

    @pl.loop(0, tiles)
    def _(i):
        for copy in weight_copies(i):
            copy.start()

    down_copy.start()
    mix_copy.start()
    barrier = pltpu.get_barrier_semaphore()

    @pl.loop(1, ep)
    def _(k):
        pl.semaphore_signal(
            barrier, inc=1, device_id={"ep": lax.rem(e + k, ep)}, device_id_type=MESH
        )

    for target in (near, far, across):
        pl.semaphore_signal(barrier, inc=1, device_id={"tp": target}, device_id_type=MESH)
    for copy in route_copies:
        copy.wait()
    slots()
    gain_copy.wait()
    token_copy.wait()
    norm()
    dispatch(e, rows.at[e, block(side, core)])
    pl.semaphore_wait(barrier, ep + 2)
    for p in count:
        gather_start(e, p)
    for k in range(1, ep):
        dispatch(targets[k], send.at[targets[k]])
        if k == 1 or not line:
            start_send(k)
        else:
            pl.when(inner == 1)(functools.partial(start_send, k))
    for copy in head_copies:
        copy.wait()
    local_part()

    @pl.when(e == 0)
    def _():
        state_in[...] = jnp.zeros_like(state_in)
        if ep > 1:
            pass_state()

    own_group(0, first=True)
    if line:
        weave(1, 0)
        far_group(0)
        arrive(2, head)
        own_group(1)

        @pl.when(inner == 0)
        def _():
            start_send(2)
            start_send(3)

        arrive(2, tail[:-1])
        relay(1)
        arrive(2, last)
        pl.when(e == 1)(state_step)
        far_group(1)
        own_group(2)

        @pl.when(inner == 0)
        def _():
            pair(1, head)
            arrive(3, most)
            relay(2)
            arrive(3, last)
            pair(1, tail)

        @pl.when(inner == 1)
        def _():
            pair(1)
            relay(2)

        far_group(2)

        @pl.when(inner == 0)
        def _():
            finish(1, head)

        @pl.when(inner == 1)
        def _():
            pair(2)
            arrive(3)
            finish(1)

        own_group(3)

        @pl.when(inner == 0)
        def _():
            pair(2, head)

        @pl.when(inner == 1)
        def _():
            finish(2)
            pl.when(e == 2)(state_step)
            memory_part()

        relay(3)
        pl.when(inner == 1)(functools.partial(pair, 0, most))
        far_group(3)

        @pl.when(inner == 0)
        def _():
            finish(1, tail)
            pair(3)
            pair(2, tail)
            finish(2, head)
            pl.when(e > 2)(state_step)
            memory_part()
            pair(0, most)
            finish(3)

        @pl.when(inner == 1)
        def _():
            pair(3)

        @pl.when(inner == 0)
        def _():
            pair(0, last)
            finish(2, tail)

        memory_relay()
        gather_back(1, first=True)
        mix_part()

        @pl.when(inner == 1)
        def _():
            finish(3, most)
            pair(0, last)
            finish(3, last)

        gather_back(2)
        finish(0, local=True)
        gather_back(0)
        drain()
        gather_back(3, last=True)
    else:
        relay(0)
        far_group(0)
        pair(0)
        finish(0, local=True)

        @pl.loop(1, ep)
        def _(j):
            arrive(j)
            own_group(j)
            relay(j)
            far_group(j)
            pl.when(e == j)(state_step)
            pair(j)
            finish(j)

        memory_part()
        memory_relay()
        mix_part()
        for k in range(ep):
            gather_back(k, k == 0, k == ep - 1)
        drain()


def on_device(
    memory_query_rows,
    memory_key_rows,
    memory_value_rows,
    input_gate_log,
    forget_gate_logits,
    forget_log_extra,
    memory_output_weight,
    second_batch_tokens,
    expert_norm_gain,
    routing_expert_index,
    routing_expert_weight,
    expert_gate_matrix,
    expert_up_matrix,
    expert_down_matrix,
):
    ep, tp = lax.axis_size("ep"), lax.axis_size("tp")
    tok_rows, width = second_batch_tokens.shape
    capacity = max(2, 5 * tok_rows * TOP // (4 * ep))
    cap = -(-capacity // GROUP) * GROUP
    part_hidden = expert_gate_matrix.shape[2]
    tiles = part_hidden // LANES
    positions = memory_query_rows.shape[0]
    heads = input_gate_log.shape[0]
    bf16 = jnp.bfloat16
    vmem = pl.BlockSpec(memory_space=pltpu.VMEM)
    hbm = pl.BlockSpec(memory_space=pl.ANY)
    whole = pltpu.SemaphoreType.DMA((ep,))
    split = pltpu.SemaphoreType.DMA((ep, len(pieces(cap))))
    state = pltpu.VMEM((heads, DH + 8, DH), jnp.float32)
    square = pltpu.VMEM((tok_rows, tok_rows), jnp.float32)
    slotted = pltpu.VMEM((ep, cap, width), bf16)
    head_rows = pltpu.VMEM(memory_query_rows.shape, bf16)
    token_rows = pltpu.VMEM((tok_rows, width), bf16)
    head_gates = pltpu.VMEM(input_gate_log.shape, jnp.float32)
    return pl.pallas_call(
        functools.partial(fused_kernel, ep, tp, cap),
        out_shape=(
            pltpu.VMEM((positions, memory_output_weight.shape[1]), bf16),
            pltpu.VMEM((tok_rows, width), bf16),
        ),
        in_specs=[hbm] * 14,
        out_specs=(vmem, vmem),
        scratch_shapes=[
            head_rows,
            head_rows,
            head_rows,
            head_gates,
            head_gates,
            head_gates,
            pltpu.VMEM((1, width), jnp.float32),
            pltpu.VMEM((TOP, tok_rows), jnp.int32),
            pltpu.VMEM((TOP, tok_rows), jnp.float32),
            token_rows,
            token_rows,
            slotted,
            square,
            square,
            square,
            pltpu.VMEM((width, 2 * part_hidden), bf16),
            pltpu.VMEM((part_hidden, width), bf16),
            pltpu.VMEM((ep, tp * cap, width), bf16),
            pltpu.VMEM((2 * cap, part_hidden), bf16),
            pltpu.VMEM((ep, tp * cap, width), bf16),
            pltpu.VMEM((ep, 2, cap, width), bf16),
            slotted,
            slotted,
            slotted,
            slotted,
            pltpu.VMEM((tok_rows, width), jnp.float32),
            state,
            state,
            state,
            pltpu.VMEM((tp, positions, heads * DH), bf16),
            pltpu.VMEM(memory_output_weight.shape, bf16),
            pltpu.SemaphoreType.DMA((2, tiles)),
            pltpu.SemaphoreType.DMA((12,)),
            pltpu.SemaphoreType.DMA((2, 1)),
            pltpu.SemaphoreType.DMA((8,)),
            split,
            split,
            split,
            split,
            whole,
            whole,
            split,
            split,
            pltpu.SemaphoreType.DMA((2, 3)),
        ],
        compiler_params=pltpu.CompilerParams(
            collective_id=0, has_side_effects=True, vmem_limit_bytes=66000000
        ),
        cost_estimate=pl.CostEstimate(
            flops=6 * ep * tp * cap * width * part_hidden,
            bytes_accessed=6 * width * part_hidden,
            transcendentals=ep * tp * cap * part_hidden,
        ),
    )(
        memory_query_rows,
        memory_key_rows,
        memory_value_rows,
        input_gate_log,
        forget_gate_logits,
        forget_log_extra,
        memory_output_weight,
        second_batch_tokens,
        expert_norm_gain.reshape(1, -1),
        routing_expert_index.T,
        routing_expert_weight.T,
        expert_gate_matrix,
        expert_up_matrix,
        expert_down_matrix,
    )


def solution(mesh):
    placed = (
        P(("grp", "ep"), "tp"),
        P(("grp", "ep"), "tp"),
        P(("grp", "ep"), "tp"),
        P("tp", ("grp", "ep")),
        P("tp", ("grp", "ep")),
        P("tp", ("grp", "ep")),
        P(None, "tp"),
        P(("grp", "ep", "tp"), None),
        P(),
        P(("grp", "ep", "tp"), None),
        P(("grp", "ep", "tp"), None),
        P("ep", None, "tp"),
        P("ep", None, "tp"),
        P("ep", "tp", None),
    )
    return jax.shard_map(
        on_device,
        mesh=mesh,
        in_specs=placed,
        out_specs=(P(("grp", "ep"), "tp"), P(("grp", "ep", "tp"), None)),
        check_vma=False,
    )
```

```python
import functools

import jax
import jax.numpy as jnp
from jax import lax
from jax.experimental import pallas as pl
from jax.experimental.pallas import tpu as pltpu
from jax.sharding import PartitionSpec as P

DH = 128
TOP = 2

rms_eps = 1e-06
highest = lax.Precision.HIGHEST


MESH = pl.DeviceIdType.MESH
LANES = 128
GROUP = 16


def pieces(cap):
    step = cap // 32 * 16
    if step == 0:
        return [(0, cap)]
    return [(at, min(step, cap - at)) for at in range(0, cap, step)]


def fused_kernel(
    ep,
    tp,
    cap,
    query_hbm,
    key_hbm,
    value_hbm,
    in_gate_hbm,
    logit_hbm,
    extra_hbm,
    mix_hbm,
    token_hbm,
    gain_hbm,
    index_hbm,
    weight_hbm,
    gate_hbm,
    up_hbm,
    down_hbm,
    mixed_ref,
    out_ref,
    query_ref,
    key_ref,
    value_ref,
    in_gate_ref,
    logit_ref,
    extra_ref,
    gain_ref,
    index_ref,
    weight_ref,
    tokens,
    normed,
    send,
    slot_row,
    slot_col,
    weight_col,
    gate_up,
    down,
    rows,
    hidden,
    part,
    near_part,
    pair_sum,
    far_part,
    result,
    returned,
    total_out,
    local_state,
    state_in,
    state_out,
    memory,
    mix,
    w_sem,
    own_sem,
    st_sem,
    sent_sem,
    z_sem,
    far_sem,
    near_sem,
    relay_sem,
    no_sem,
    nf_sem,
    fp_sem,
    r_sem,
    m_sem,
):
    e = lax.axis_index("ep")
    t = lax.axis_index("tp")
    side, core = t // 2, t % 2
    near = side * 2 + (1 - core)
    far = (1 - side) * 2 + core
    across = (1 - side) * 2 + (1 - core)
    heads = in_gate_ref.shape[0]
    length = in_gate_ref.shape[1]
    tiles = gate_up.shape[1] // (2 * LANES)
    width = rows.shape[2]
    part_hidden = down.shape[0]
    tok_rows = tokens.shape[0]
    cuts = pieces(cap)
    count = range(len(cuts))
    head, tail = count[:1], count[1:]
    most, last = count[:-1], count[-1:]
    line = ep == 4 and len(cuts) > 1

    if line:
        left = 1 - e // 2
        inner = e * left + (3 - e) * (1 - left)

        def seat(v):
            return v * left + (3 - v) * (1 - left)

        targets = [e, seat(1 + 2 * inner), seat(3 - inner), seat(2 - 2 * inner)]
        sources = [e, seat(2 - 2 * inner), seat(1 + inner), seat(3)]

        def source(j):
            return sources[j]

        gathers = [e, seat(1 + 2 * inner), seat(3 - inner), seat(2 - 2 * inner)]
    else:
        targets = [lax.rem(e + k, ep) for k in range(ep)]
        gathers = targets

        def source(j):
            return lax.rem(e + ep - j, ep)

    def block(side_at, core_at, p=None):
        off, size = (0, cap) if p is None else cuts[p]
        return pl.ds(pl.multiple_of((side_at * 2 + core_at) * cap + off, GROUP), size)

    def cut(p):
        return pl.ds(cuts[p][0], cuts[p][1])

    def remote(src, dst, sent, received, target):
        return pltpu.make_async_remote_copy(
            src_ref=src,
            dst_ref=dst,
            send_sem=sent,
            recv_sem=received,
            device_id=target,
            device_id_type=MESH,
        )

    def pair_cols(i, which):
        return pl.ds(pl.multiple_of((2 * i + which) * LANES, LANES), LANES)

    def weight_copies(i):
        cols = pl.ds(pl.multiple_of(i * LANES, LANES), LANES)
        return (
            pltpu.make_async_copy(
                gate_hbm.at[0, :, cols], gate_up.at[:, pair_cols(i, 0)], w_sem.at[0, i]
            ),
            pltpu.make_async_copy(
                up_hbm.at[0, :, cols], gate_up.at[:, pair_cols(i, 1)], w_sem.at[1, i]
            ),
        )

    token_copy = pltpu.make_async_copy(token_hbm, tokens, own_sem.at[0])
    down_copy = pltpu.make_async_copy(down_hbm.at[0], down, own_sem.at[1])
    mix_copy = pltpu.make_async_copy(mix_hbm, mix, own_sem.at[2])
    head_copies = [
        pltpu.make_async_copy(query_hbm, query_ref, own_sem.at[3]),
        pltpu.make_async_copy(key_hbm, key_ref, own_sem.at[4]),
        pltpu.make_async_copy(value_hbm, value_ref, own_sem.at[5]),
        pltpu.make_async_copy(in_gate_hbm, in_gate_ref, own_sem.at[6]),
        pltpu.make_async_copy(logit_hbm, logit_ref, own_sem.at[7]),
        pltpu.make_async_copy(extra_hbm, extra_ref, own_sem.at[8]),
    ]
    route_copies = [
        pltpu.make_async_copy(index_hbm, index_ref, own_sem.at[9]),
        pltpu.make_async_copy(weight_hbm, weight_ref, own_sem.at[10]),
    ]
    gain_copy = pltpu.make_async_copy(gain_hbm, gain_ref, own_sem.at[11])

    def z_send(s, p):
        return remote(
            send.at[s, cut(p)], rows.at[e, block(side, core, p)],
            sent_sem.at[0], z_sem.at[e, p], {"ep": s},
        )

    def z_recv(s, p):
        return remote(
            send.at[s, cut(p)], rows.at[s, block(side, core, p)],
            sent_sem.at[0], z_sem.at[s, p], {"ep": s},
        )

    def far_copy(s, p):
        span = rows.at[s, block(side, core, p)]
        return remote(span, span, sent_sem.at[1], far_sem.at[s, p], {"tp": far})

    def near_copy(s, p):
        span = rows.at[s, block(side, core, p)]
        return remote(span, span, sent_sem.at[2], near_sem.at[s, p], {"tp": near})

    def relay_copy(s, p):
        span = rows.at[s, block(1 - side, core, p)]
        return remote(span, span, sent_sem.at[3], relay_sem.at[s, p], {"tp": near})

    def near_own_copy(s):
        return remote(
            part.at[s, block(side, 1 - core)], near_part.at[s, 0],
            sent_sem.at[4], no_sem.at[s], {"tp": near},
        )

    def stretch(which):
        start = cuts[which[0]][0]
        return start, sum(cuts[p][1] for p in which)

    def near_far_copy(s, which):
        start, size = stretch(which)
        base = ((1 - side) * 2 + 1 - core) * cap + start
        return remote(
            part.at[s, pl.ds(pl.multiple_of(base, GROUP), size)],
            near_part.at[s, 1, pl.ds(start, size)],
            sent_sem.at[5], nf_sem.at[s, which[0]], {"tp": near},
        )

    def far_part_copy(s, p):
        return remote(
            pair_sum.at[s, cut(p)], far_part.at[s, cut(p)],
            sent_sem.at[6], fp_sem.at[s, p], {"tp": far},
        )

    def return_send(s, p):
        return remote(
            result.at[s, cut(p)], returned.at[e, cut(p)],
            sent_sem.at[7], r_sem.at[e, p], {"ep": s},
        )

    def return_recv(s, p):
        return remote(
            result.at[s, cut(p)], returned.at[s, cut(p)],
            sent_sem.at[7], r_sem.at[s, p], {"ep": s},
        )

    state_copy = remote(
        state_out, state_in, st_sem.at[0, 0], st_sem.at[1, 0], {"ep": lax.rem(e + 1, ep)}
    )

    def memory_copy(i):
        span = memory.at[far if i == 2 else t]
        return remote(
            span, span, m_sem.at[0, i], m_sem.at[1, i], {"tp": far if i == 1 else near}
        )

    def gates(h):
        logits = logit_ref[h : h + 1, :]
        forget = (
            jnp.minimum(logits, 0.0) - jnp.log1p(jnp.exp(-jnp.abs(logits)))
        ) + extra_ref[h : h + 1, :]
        at_row = lax.broadcasted_iota(jnp.int32, (length, length), 0)
        at_col = lax.broadcasted_iota(jnp.int32, (length, length), 1)
        diagonal = at_row == at_col
        in_row = in_gate_ref[h : h + 1, :]
        in_col = jnp.sum(jnp.where(diagonal, in_row, 0.0), axis=1, keepdims=True)
        sum_col = jnp.sum(jnp.where(at_col <= at_row, forget, 0.0), axis=1, keepdims=True)
        sum_row = jnp.sum(jnp.where(diagonal, sum_col, 0.0), axis=0, keepdims=True)
        total = jnp.sum(forget, axis=1, keepdims=True)
        return in_row, in_col, sum_row, sum_col, total, at_col <= at_row

    def heads_of(ref, h):
        return ref[:, h * DH : (h + 1) * DH].astype(jnp.float32)

    def local_part():
        for h in range(heads):
            _, in_col, _, sum_col, total, _ = gates(h)
            weights = total - sum_col + in_col
            stab = jnp.max(weights, axis=0, keepdims=True)
            weighted = jnp.exp(weights - stab) * (heads_of(key_ref, h) * DH ** (-0.5))
            local_state[h, 0:DH, :] = jnp.dot(
                weighted.T, heads_of(value_ref, h), precision=highest,
                preferred_element_type=jnp.float32,
            )
            local_state[h, DH : DH + 1, :] = jnp.sum(weighted, axis=0, keepdims=True)
            local_state[h, DH + 1 : DH + 2, :] = jnp.broadcast_to(stab, (1, DH))
            local_state[h, DH + 2 : DH + 3, :] = jnp.broadcast_to(total, (1, DH))

    def pass_state():
        for h in range(heads):
            total = local_state[h, DH + 2 : DH + 3, :]
            stab_own = local_state[h, DH + 1 : DH + 2, :]
            carried = total + state_in[h, DH + 1 : DH + 2, :]
            stab = jnp.maximum(carried, stab_own)
            old, new = jnp.exp(carried - stab), jnp.exp(stab_own - stab)
            state_out[h, 0 : DH + 1, :] = (
                old * state_in[h, 0 : DH + 1, :] + new * local_state[h, 0 : DH + 1, :]
            )
            state_out[h, DH + 1 : DH + 2, :] = stab
        state_copy.start()

    def memory_part():
        for h in range(heads):
            in_row, _, sum_row, sum_col, _, causal = gates(h)
            decays = jnp.where(causal, sum_col - sum_row + in_row, -jnp.inf)
            carried_max = sum_col + state_in[h, DH + 1 : DH + 2, 0:1]
            row_max = jnp.maximum(jnp.max(decays, axis=1, keepdims=True), carried_max)
            queries = heads_of(query_ref, h)
            keys = heads_of(key_ref, h) * DH ** (-0.5)
            scores = jnp.dot(
                queries, keys.T, precision=highest, preferred_element_type=jnp.float32
            ) * jnp.exp(decays - row_max)
            carried = jnp.exp(carried_max - row_max)
            numerator = carried * jnp.dot(
                queries, state_in[h, 0:DH, :], precision=highest,
                preferred_element_type=jnp.float32,
            ) + jnp.dot(
                scores, heads_of(value_ref, h), precision=highest,
                preferred_element_type=jnp.float32,
            )
            denominator = carried * jnp.sum(
                queries * state_in[h, DH : DH + 1, :], axis=1, keepdims=True
            ) + jnp.sum(scores, axis=1, keepdims=True)
            memory[t, :, h * DH : (h + 1) * DH] = (
                numerator / jnp.maximum(jnp.abs(denominator), jnp.exp(-row_max))
            ).astype(jnp.bfloat16)
        memory_copy(0).start()
        memory_copy(1).start()

    def memory_relay():
        memory_copy(1).wait_recv()
        memory_copy(2).start()

    def mix_part():
        mix_copy.wait()
        memory_copy(0).wait_recv()
        memory_copy(2).wait_recv()
        total = jnp.zeros(mixed_ref.shape, jnp.float32)
        for i in range(tp):
            total = total + jnp.dot(
                memory[i], mix[i * heads * DH : (i + 1) * heads * DH, :],
                preferred_element_type=jnp.float32,
            )
        mixed_ref[...] = total.astype(jnp.bfloat16)

    def slots():
        at_row = lax.broadcasted_iota(jnp.int32, (tok_rows, tok_rows), 0)
        at_col = lax.broadcasted_iota(jnp.int32, (tok_rows, tok_rows), 1)
        chosen = [index_ref[c : c + 1, :] == at_row for c in range(TOP)]
        member = jnp.zeros((tok_rows, tok_rows), jnp.float32)
        weights = jnp.zeros((tok_rows, tok_rows), jnp.float32)
        for c in range(TOP):
            member = member + jnp.where(chosen[c], 1.0, 0.0)
            weights = weights + jnp.where(chosen[c], weight_ref[c : c + 1, :], 0.0)
        earlier = jnp.where(at_row < at_col, 1.0, 0.0).astype(jnp.bfloat16)
        ranks = jnp.dot(member.astype(jnp.bfloat16), earlier, preferred_element_type=jnp.float32)
        slot = jnp.where(member > 0.0, ranks, -1.0)
        slot_row[...] = slot
        slot_col[...] = slot.T
        weight_col[...] = weights.T

    def norm():
        @pl.loop(0, tok_rows // GROUP, unroll=4)
        def _(i):
            span = pl.ds(pl.multiple_of(i * GROUP, GROUP), GROUP)
            values = tokens[span].astype(jnp.float32)
            scale = lax.rsqrt(jnp.mean(values * values, axis=1, keepdims=True) + rms_eps)
            normed[span] = (values * scale * gain_ref[...]).astype(jnp.bfloat16)

    def dispatch(x, place):
        at_slot = lax.broadcasted_iota(jnp.int32, (cap, tok_rows), 0).astype(jnp.float32)
        taken = jnp.where(at_slot == slot_row[pl.ds(x, 1), :], 1.0, 0.0).astype(jnp.bfloat16)

        place[...] = jnp.dot(
            taken, normed[...], preferred_element_type=jnp.float32
        ).astype(jnp.bfloat16)

    def combine(x, first, last):
        lane = lax.broadcasted_iota(jnp.int32, (tok_rows, tok_rows), 1)
        slot = jnp.sum(jnp.where(lane == x, slot_col[...], 0.0), axis=1, keepdims=True)
        weight = jnp.sum(jnp.where(lane == x, weight_col[...], 0.0), axis=1, keepdims=True)
        at_slot = lax.broadcasted_iota(jnp.int32, (tok_rows, cap), 1).astype(jnp.float32)
        taken = jnp.where(at_slot == slot, 1.0, 0.0).astype(jnp.bfloat16)

        total = weight * jnp.dot(taken, returned[x], preferred_element_type=jnp.float32)
        if not first:
            total = total + total_out[...]
        if last:
            out_ref[...] = total.astype(jnp.bfloat16)
        else:
            total_out[...] = total

    def feed_forward(s, spans, first=False):
        size = sum(span.size for span in spans)
        step = 4 * LANES
        if len(spans) > 1:
            taken = jnp.concatenate([rows[s, span] for span in spans], axis=0)
        for start in range(0, 2 * part_hidden, step):
            stop = min(start + step, 2 * part_hidden)
            if first:
                for i in range(start // (2 * LANES), stop // (2 * LANES)):
                    for copy in weight_copies(i):
                        copy.wait()
            both = jnp.dot(
                taken if len(spans) > 1 else rows[s, spans[0]], gate_up[:, start:stop],
                preferred_element_type=jnp.float32,
            )
            for i in range(0, stop - start, 2 * LANES):
                act, up_act = both[:, i : i + LANES], both[:, i + LANES : i + 2 * LANES]
                at = (start + i) // 2
                hidden[0:size, at : at + LANES] = (
                    jax.nn.silu(act) * up_act
                ).astype(jnp.bfloat16)
        if first:
            down_copy.wait()
        made = jnp.dot(
            hidden[0:size], down[...], preferred_element_type=jnp.float32
        ).astype(jnp.bfloat16)
        done = 0
        for span in spans:
            part[s, span] = made[done : done + span.size]
            done += span.size

    def chip_rows(group):
        return pl.ds(pl.multiple_of(group * 2 * cap, 2 * cap), 2 * cap)

    def gather_start(s, p):
        far_copy(s, p).start()
        near_copy(s, p).start()

    def arrive(j, which=None):
        for p in count if which is None else which:
            z_recv(source(j), p).wait_recv()
            gather_start(source(j), p)

    def weave(j, k):
        for p in most:
            arrive(j, [p])
            relay(k, [p])
        relay(k, last)
        arrive(j, last)

    def own_group(j, first=False):
        s = source(j)
        for p in count:
            near_copy(s, p).wait_recv()
        feed_forward(s, [chip_rows(side)], first=first)
        near_own_copy(s).start()

    def relay(j, which=None):
        s = source(j)
        for p in count if which is None else which:
            far_copy(s, p).wait_recv()
            relay_copy(s, p).start()

    def far_group(j):
        s = source(j)
        for p in count:
            relay_copy(s, p).wait_recv()
        feed_forward(s, [chip_rows(1 - side)])
        near_far_copy(s, count).start()

    def far_cut(j, which):
        s = source(j)
        for p in which:
            relay_copy(s, p).wait_recv()
        start, size = stretch(which)
        base = (1 - side) * 2 * cap + start
        feed_forward(
            s, [pl.ds(pl.multiple_of(base + c * cap, GROUP), size) for c in range(2)]
        )
        near_far_copy(s, which).start()

    def pair(j, which=None, cut_at=None):
        s = source(j)
        base = (1 - side) * 2 * cap + core * cap
        for p in count if which is None else which:
            if p == 0:
                near_far_copy(s, count if cut_at is None else count[:cut_at]).wait_recv()
            elif p == cut_at:
                near_far_copy(s, count[cut_at:]).wait_recv()
            off, size = cuts[p]

            @pl.loop(0, size // GROUP)
            def _(i):
                at = pl.multiple_of(off + i * GROUP, GROUP)
                pair_sum[s, pl.ds(at, GROUP)] = (
                    part[s, pl.ds(pl.multiple_of(base + at, GROUP), GROUP)].astype(jnp.float32)
                    + near_part[s, 1, pl.ds(at, GROUP)].astype(jnp.float32)
                ).astype(jnp.bfloat16)

            far_part_copy(s, p).start()

    def finish(j, which=None, local=False):
        s = source(j)
        base = side * 2 * cap + core * cap
        for p in count if which is None else which:
            if p == 0:
                near_own_copy(s).wait_recv()
            far_part_copy(s, p).wait_recv()
            off, size = cuts[p]

            @pl.loop(0, size // GROUP)
            def _(i):
                at = pl.multiple_of(off + i * GROUP, GROUP)
                total = (
                    part[s, pl.ds(pl.multiple_of(base + at, GROUP), GROUP)].astype(jnp.float32)
                    + near_part[s, 0, pl.ds(at, GROUP)].astype(jnp.float32)
                    + far_part[s, pl.ds(at, GROUP)].astype(jnp.float32)
                ).astype(jnp.bfloat16)
                if local:
                    returned[s, pl.ds(at, GROUP)] = total
                else:
                    result[s, pl.ds(at, GROUP)] = total

            if not local:
                return_send(s, p).start()

    def gather_back(k, first=False, last=False):
        x = gathers[k]
        if k > 0:
            for p in count:
                return_recv(x, p).wait_recv()
        combine(x, first, last)

    def start_send(k):
        for p in count:
            z_send(targets[k], p).start()

    def drain():
        for i in range(3):
            memory_copy(i).wait_send()

        @pl.when(e + 1 < ep)
        def _():
            state_copy.wait_send()

        for k in range(8):
            stages = ep - 1 if k in (0, 7) else ep
            if stages:
                span = send.at[pl.ds(0, stages)]
                remote(
                    span, span, sent_sem.at[k], no_sem.at[0], {"tp": near}
                ).wait_send()

    def state_step():
        state_copy.wait_recv()

        @pl.when(e + 1 < ep)
        def _():
            pass_state()

    for copy in route_copies:
        copy.start()
    token_copy.start()
    gain_copy.start()
    for copy in head_copies:
        copy.start()

    @pl.loop(0, tiles)
    def _(i):
        for copy in weight_copies(i):
            copy.start()

    down_copy.start()
    mix_copy.start()
    barrier = pltpu.get_barrier_semaphore()

    @pl.loop(1, ep)
    def _(k):
        pl.semaphore_signal(
            barrier, inc=1, device_id={"ep": lax.rem(e + k, ep)}, device_id_type=MESH
        )

    for target in (near, far, across):
        pl.semaphore_signal(barrier, inc=1, device_id={"tp": target}, device_id_type=MESH)
    for copy in route_copies:
        copy.wait()
    slots()
    gain_copy.wait()
    token_copy.wait()
    norm()
    dispatch(e, rows.at[e, block(side, core)])
    pl.semaphore_wait(barrier, ep + 2)
    for p in count:
        gather_start(e, p)
    for k in range(1, ep):
        dispatch(targets[k], send.at[targets[k]])
        if k == 1 or not line:
            start_send(k)
        else:
            pl.when(inner == 1)(functools.partial(start_send, k))
    for copy in head_copies:
        copy.wait()
    local_part()

    @pl.when(e == 0)
    def _():
        state_in[...] = jnp.zeros_like(state_in)
        if ep > 1:
            pass_state()

    own_group(0, first=True)
    if line:
        weave(1, 0)
        far_group(0)
        arrive(2, head)
        own_group(1)

        @pl.when(inner == 0)
        def _():
            start_send(2)
            start_send(3)

        arrive(2, tail[:-1])
        relay(1)
        arrive(2, last)
        pl.when(e == 1)(state_step)
        far_group(1)
        own_group(2)

        @pl.when(inner == 0)
        def _():
            pair(1, head)
            arrive(3, most)
            relay(2)
            arrive(3, last)
            pair(1, tail)

        @pl.when(inner == 1)
        def _():
            pair(1)
            relay(2)

        far_group(2)

        @pl.when(inner == 0)
        def _():
            finish(1, head)

        @pl.when(inner == 1)
        def _():
            pair(2)
            arrive(3)
            finish(1)

        own_group(3)

        @pl.when(inner == 0)
        def _():
            pair(2, head)

        @pl.when(inner == 1)
        def _():
            finish(2)
            pl.when(e == 2)(state_step)
            memory_part()

        relay(3, head)
        far_cut(3, head)
        pl.when(inner == 1)(functools.partial(pair, 0, head))
        relay(3, tail)
        pair(3, head, cut_at=1)
        far_cut(3, tail)

        @pl.when(inner == 0)
        def _():
            finish(1, tail)
            pair(3, tail, cut_at=1)
            pair(2, tail)
            finish(2, head)
            pl.when(e > 2)(state_step)
            memory_part()
            pair(0, most)
            finish(3)
            pair(0, last)
            finish(2, tail)

        pl.when(inner == 1)(functools.partial(pair, 3, tail, 1))
        memory_relay()
        gather_back(1, first=True)
        mix_part()

        @pl.when(inner == 1)
        def _():
            finish(3, head)
            pair(0, tail)
            finish(3, tail)

        gather_back(2)
        finish(0, local=True)
        gather_back(0)
        drain()
        gather_back(3, last=True)
    else:
        relay(0)
        far_group(0)
        pair(0)
        finish(0, local=True)

        @pl.loop(1, ep)
        def _(j):
            arrive(j)
            own_group(j)
            relay(j)
            far_group(j)
            pl.when(e == j)(state_step)
            pair(j)
            finish(j)

        memory_part()
        memory_relay()
        mix_part()
        for k in range(ep):
            gather_back(k, k == 0, k == ep - 1)
        drain()


def on_device(
    memory_query_rows,
    memory_key_rows,
    memory_value_rows,
    input_gate_log,
    forget_gate_logits,
    forget_log_extra,
    memory_output_weight,
    second_batch_tokens,
    expert_norm_gain,
    routing_expert_index,
    routing_expert_weight,
    expert_gate_matrix,
    expert_up_matrix,
    expert_down_matrix,
):
    ep, tp = lax.axis_size("ep"), lax.axis_size("tp")
    tok_rows, width = second_batch_tokens.shape
    capacity = max(2, 5 * tok_rows * TOP // (4 * ep))
    cap = -(-capacity // GROUP) * GROUP
    part_hidden = expert_gate_matrix.shape[2]
    tiles = part_hidden // LANES
    positions = memory_query_rows.shape[0]
    heads = input_gate_log.shape[0]
    bf16 = jnp.bfloat16
    vmem = pl.BlockSpec(memory_space=pltpu.VMEM)
    hbm = pl.BlockSpec(memory_space=pl.ANY)
    whole = pltpu.SemaphoreType.DMA((ep,))
    split = pltpu.SemaphoreType.DMA((ep, len(pieces(cap))))
    state = pltpu.VMEM((heads, DH + 8, DH), jnp.float32)
    square = pltpu.VMEM((tok_rows, tok_rows), jnp.float32)
    slotted = pltpu.VMEM((ep, cap, width), bf16)
    head_rows = pltpu.VMEM(memory_query_rows.shape, bf16)
    token_rows = pltpu.VMEM((tok_rows, width), bf16)
    head_gates = pltpu.VMEM(input_gate_log.shape, jnp.float32)
    return pl.pallas_call(
        functools.partial(fused_kernel, ep, tp, cap),
        out_shape=(
            pltpu.VMEM((positions, memory_output_weight.shape[1]), bf16),
            pltpu.VMEM((tok_rows, width), bf16),
        ),
        in_specs=[hbm] * 14,
        out_specs=(vmem, vmem),
        scratch_shapes=[
            head_rows,
            head_rows,
            head_rows,
            head_gates,
            head_gates,
            head_gates,
            pltpu.VMEM((1, width), jnp.float32),
            pltpu.VMEM((TOP, tok_rows), jnp.int32),
            pltpu.VMEM((TOP, tok_rows), jnp.float32),
            token_rows,
            token_rows,
            slotted,
            square,
            square,
            square,
            pltpu.VMEM((width, 2 * part_hidden), bf16),
            pltpu.VMEM((part_hidden, width), bf16),
            pltpu.VMEM((ep, tp * cap, width), bf16),
            pltpu.VMEM((2 * cap, part_hidden), bf16),
            pltpu.VMEM((ep, tp * cap, width), bf16),
            pltpu.VMEM((ep, 2, cap, width), bf16),
            slotted,
            slotted,
            slotted,
            slotted,
            pltpu.VMEM((tok_rows, width), jnp.float32),
            state,
            state,
            state,
            pltpu.VMEM((tp, positions, heads * DH), bf16),
            pltpu.VMEM(memory_output_weight.shape, bf16),
            pltpu.SemaphoreType.DMA((2, tiles)),
            pltpu.SemaphoreType.DMA((12,)),
            pltpu.SemaphoreType.DMA((2, 1)),
            pltpu.SemaphoreType.DMA((8,)),
            split,
            split,
            split,
            split,
            whole,
            split,
            split,
            split,
            pltpu.SemaphoreType.DMA((2, 3)),
        ],
        compiler_params=pltpu.CompilerParams(
            collective_id=0, has_side_effects=True, vmem_limit_bytes=66000000
        ),
        cost_estimate=pl.CostEstimate(
            flops=6 * ep * tp * cap * width * part_hidden,
            bytes_accessed=6 * width * part_hidden,
            transcendentals=ep * tp * cap * part_hidden,
        ),
    )(
        memory_query_rows,
        memory_key_rows,
        memory_value_rows,
        input_gate_log,
        forget_gate_logits,
        forget_log_extra,
        memory_output_weight,
        second_batch_tokens,
        expert_norm_gain.reshape(1, -1),
        routing_expert_index.T,
        routing_expert_weight.T,
        expert_gate_matrix,
        expert_up_matrix,
        expert_down_matrix,
    )


def solution(mesh):
    placed = (
        P(("grp", "ep"), "tp"),
        P(("grp", "ep"), "tp"),
        P(("grp", "ep"), "tp"),
        P("tp", ("grp", "ep")),
        P("tp", ("grp", "ep")),
        P("tp", ("grp", "ep")),
        P(None, "tp"),
        P(("grp", "ep", "tp"), None),
        P(),
        P(("grp", "ep", "tp"), None),
        P(("grp", "ep", "tp"), None),
        P("ep", None, "tp"),
        P("ep", None, "tp"),
        P("ep", "tp", None),
    )
    return jax.shard_map(
        on_device,
        mesh=mesh,
        in_specs=placed,
        out_specs=(P(("grp", "ep"), "tp"), P(("grp", "ep", "tp"), None)),
        check_vma=False,
    )
```
